128 devices in a mesh: sp: 16 (over z, x), tp: 4 (over y), dp: 2 (over core).
Axes of the slice: x: 4, y: 4, z: 4, core: 2. Of those that a mesh axis runs over, the one named last changes fastest.
Arguments:
- latent: bfloat16 [8192, 4, 2048], P(('sp', 'tp'), 'dp'), may hold values from -6 to 6
- context: bfloat16 [1024, 4, 2048], P('sp', 'dp'), may hold values from -6 to 6
- condition: bfloat16 [4, 2048], P('dp', 'sp'), may hold values from -6 to 6
- ctx_condition: bfloat16 [2048], P('sp'), may hold values from -6 to 6
- norm_gain: float32 [2048], replicated, may hold values from 0.1 to 1.9
- w_shift: bfloat16 [2048, 2048], P('sp', 'tp'), may hold values from -0.1875 to 0.1875
- w_scale: bfloat16 [2048, 2048], P('sp', 'tp'), may hold values from -0.1875 to 0.1875
- w_gate: bfloat16 [2048, 2048], P('sp', 'tp'), may hold values from -0.1875 to 0.1875
- w_query: bfloat16 [2048, 2048], P(None, 'tp'), may hold values from -0.125 to 0.125
- w_key: bfloat16 [2048, 512], P(None, 'tp'), may hold values from -6 to 6
- w_value: bfloat16 [2048, 512], P(None, 'tp'), may hold values from -0.125 to 0.125
- w_out: bfloat16 [2048, 2048], P('tp'), may hold values from -1 to 1
- sink: float32 [16], P('tp'), may hold values from 5 to 9
Outputs:
- mixed: bfloat16 [8192, 4, 2048], P(('sp', 'tp'), 'dp')
The draws below stay inside these ranges and needn't reach their ends.
All inputs are finite; a program needn't handle non-finite values.
Results may differ from the reference program's by a relative error of at most 0.015.
The reference program's roundings to bfloat16 on the way count: a program that leaves them out, or rounds other values in their place, can miss the bound.
Values may be sent and summed in bfloat16 or wider, within the bound.
No kernel may reach another device: no remote copies, remote signals or barrier semaphores. Data moves between devices by JAX's collectives and lax.ppermute only.
A program may use at most 128 MiB of HBM per device.

```python
import jax
import jax.numpy as jnp
from jax import lax

D = 2048
HEADS = 16
KV_HEADS = 4
HEAD_DIM = 128
WINDOW = 128
GRID_W = 64
CTX = 1024
TOK_SP = 512
SEQ = 8192
SAMPLES = 4
N_SP = 16
N_TP = 4


def draw_w_key(key, part):
    matrix = jax.random.normal(key, (D, KV_HEADS * HEAD_DIM), jnp.float32) * D ** (-0.5)
    return jnp.clip(matrix, -6.0, 6.0).astype(jnp.bfloat16)


def block_levels(rng, shape, split, low, high):
    level = 1.0
    for dim, shards_of in split:
        draws = jax.random.uniform(jax.random.fold_in(jax.random.fold_in(rng, 6), dim), (shards_of,), jnp.float32, low / len(split), high / len(split))
        level = level * jnp.repeat(jnp.exp(draws), shape[dim] // shards_of).reshape((-1,) + (1,) * (len(shape) - 1 - dim))
    return level


def gaussian(key, dims, scale, reach, cuts=(), held_as=jnp.bfloat16):
    array = jax.random.normal(key, dims, jnp.float32) * scale
    if len(cuts) > 0:
        array = block_levels(key, dims, cuts, -0.22, 0.18) * array
    return jnp.clip(array, min=-reach, max=reach).astype(held_as)


def setup_inputs(seed: int = 0) -> dict:
    key_list = jax.random.split(jax.random.key(seed), 14)
    return {
        "latent": gaussian(key_list[0], (SEQ, SAMPLES, D), 1.0, 6.0, ((0, 64), (1, 2))),
        "context": gaussian(key_list[1], (CTX, SAMPLES, D), 1.0, 6.0, ((0, 16), (1, 2))),
        "condition": gaussian(key_list[2], (SAMPLES, D), 1.0, 6.0, ((0, 2), (1, 16))),
        "ctx_condition": gaussian(key_list[3], (D,), 1.0, 6.0, ((0, 16),)),
        "norm_gain": jnp.clip(1.0 + 0.18 * jax.random.normal(key_list[4], (D,), jnp.float32), 0.1, 1.9),
        "w_shift": gaussian(key_list[5], (D, D), (D // 2) ** -0.5, 0.1875, ((0, 16), (1, 4))),
        "w_scale": gaussian(key_list[6], (D, D), (D // 2) ** -0.5, 0.1875, ((0, 16), (1, 4))),
        "w_gate": gaussian(key_list[7], (D, D), (D // 2) ** -0.5, 0.1875, ((0, 16), (1, 4))),
        "w_query": gaussian(key_list[8], (D, HEADS * HEAD_DIM), D ** -0.5, 0.125, ((1, 4),)),
        "w_key": draw_w_key(jax.random.fold_in(key_list[13], 71), 0),
        "w_value": gaussian(key_list[10], (D, KV_HEADS * HEAD_DIM), D ** -0.5, 0.125, ((1, 4),)),
        "w_out": gaussian(key_list[11], (HEADS * HEAD_DIM, D), (HEAD_DIM // 4) ** -0.5, 1.0, ((0, 4),)),
        "sink": jnp.clip(5.0 + 4.0 * jax.random.uniform(key_list[12], (HEADS,), jnp.float32) ** block_levels(key_list[12], (HEADS,), ((0, 4),), -0.2, 0.2), 5.0, 9.0),
    }


EPSILON = 1e-06
NEGATIVE = -1e+30

def normed(values, gain):
    floats = values.astype(jnp.float32)
    return floats * lax.rsqrt(lax.optimization_barrier(jnp.mean(floats * floats, axis=-1, keepdims=True)) + EPSILON) * gain

def rotate(tensor, position):
    quarter = HEAD_DIM // 4
    freqs = 10000.0 ** (-jnp.arange(quarter, dtype=jnp.float32) / quarter)
    row_pos = (position // GRID_W).astype(jnp.float32)
    col_pos = (position % GRID_W).astype(jnp.float32)
    angle = jnp.stack([row_pos[:, None] * freqs, col_pos[:, None] * freqs], axis=1)
    cosine = jnp.cos(angle)[:, None, None]
    sine = jnp.sin(angle)[:, None, None]
    pieces = tensor.reshape(tensor.shape[:-1] + (2, 2, quarter))
    first = pieces[..., 0, :]
    second = pieces[..., 1, :]
    turned = jnp.stack([first * cosine - second * sine, second * cosine + first * sine], axis=-2)
    return turned.reshape(tensor.shape)

def attend_block(queries, keys, values, allowed, ctx_keys, ctx_values, sink_logit):
    q_rows, batch, heads_n, width = queries.shape
    kv_heads = keys.shape[2]
    grouped = queries.reshape(q_rows, batch, kv_heads, heads_n // kv_heads, width).astype(jnp.float32)
    factor = width ** (-0.5)
    local_scores = jnp.einsum('qbkgd,jbkd->bkgqj', grouped, keys.astype(jnp.float32)) * factor
    local_scores = jnp.where(allowed, local_scores, NEGATIVE)
    ctx_scores = jnp.einsum('qbkgd,jbkd->bkgqj', grouped, ctx_keys.astype(jnp.float32)) * factor
    sink_scores = sink_logit.astype(jnp.float32).reshape(kv_heads, heads_n // kv_heads)[None, :, :, None, None]
    top = jnp.maximum(jnp.maximum(lax.optimization_barrier(jnp.max(local_scores, axis=-1, keepdims=True)), lax.optimization_barrier(jnp.max(ctx_scores, axis=-1, keepdims=True))), sink_scores)
    local_exp = jnp.exp(local_scores - top)
    ctx_exp = jnp.exp(ctx_scores - top)
    total = lax.optimization_barrier(jnp.sum(local_exp, axis=-1, keepdims=True)) + lax.optimization_barrier(jnp.sum(ctx_exp, axis=-1, keepdims=True)) + jnp.exp(sink_scores - top)
    local_weights = (local_exp / total).astype(jnp.bfloat16)
    ctx_weights = (ctx_exp / total).astype(jnp.bfloat16)
    result = jnp.einsum('bkgqj,jbkd->qbkgd', local_weights.astype(jnp.float32), values.astype(jnp.float32))
    result = result + jnp.einsum('bkgqj,jbkd->qbkgd', ctx_weights.astype(jnp.float32), ctx_values.astype(jnp.float32))
    return result.astype(jnp.bfloat16).reshape(q_rows, batch, heads_n * width)

def reference(latent, context, condition, ctx_condition, norm_gain, w_shift, w_scale, w_gate, w_query, w_key, w_value, w_out, sink):
    act = jax.nn.silu(condition.astype(jnp.float32)).astype(jnp.bfloat16)
    ctx_act = jax.nn.silu(ctx_condition.astype(jnp.float32)).astype(jnp.bfloat16)
    both = jnp.concatenate([act, ctx_act[None]], axis=0)
    shift_all = jnp.dot(both, w_shift, preferred_element_type=jnp.float32)
    scale_all = jnp.dot(both, w_scale, preferred_element_type=jnp.float32)
    gate = jnp.dot(act, w_gate, preferred_element_type=jnp.float32)
    samples_n = latent.shape[1]
    hidden = (normed(latent, norm_gain) * (1.0 + scale_all[None, :samples_n]) + shift_all[None, :samples_n]).astype(jnp.bfloat16)
    ctx_hidden = (normed(context, norm_gain) * (1.0 + scale_all[samples_n]) + shift_all[samples_n]).astype(jnp.bfloat16)
    seq_len = latent.shape[0]
    position = jnp.arange(seq_len, dtype=jnp.int32)
    queries = jnp.dot(hidden, w_query, preferred_element_type=jnp.float32).reshape(seq_len, samples_n, HEADS, HEAD_DIM)
    queries = rotate(queries, position).astype(jnp.bfloat16)
    keys = jnp.dot(hidden, w_key, preferred_element_type=jnp.float32).reshape(seq_len, samples_n, KV_HEADS, HEAD_DIM)
    keys = rotate(keys, position).astype(jnp.bfloat16)
    values = jnp.dot(hidden, w_value, preferred_element_type=jnp.float32).astype(jnp.bfloat16).reshape(seq_len, samples_n, KV_HEADS, HEAD_DIM)
    ctx_keys = jnp.dot(ctx_hidden, w_key, preferred_element_type=jnp.float32).astype(jnp.bfloat16).reshape(CTX, samples_n, KV_HEADS, HEAD_DIM)
    ctx_values = jnp.dot(ctx_hidden, w_value, preferred_element_type=jnp.float32).astype(jnp.bfloat16).reshape(CTX, samples_n, KV_HEADS, HEAD_DIM)
    padding = ((WINDOW, WINDOW), (0, 0), (0, 0), (0, 0))
    keys_pad = jnp.pad(keys, padding)
    values_pad = jnp.pad(values, padding)
    span = TOK_SP + 2 * WINDOW

    def one_block(block):
        start = (block * TOK_SP).astype(jnp.int32)
        block_q = lax.dynamic_slice_in_dim(queries, start, TOK_SP, 0)
        block_k = lax.dynamic_slice_in_dim(keys_pad, start, span, 0)
        block_v = lax.dynamic_slice_in_dim(values_pad, start, span, 0)
        q_pos = start + jnp.arange(TOK_SP, dtype=jnp.int32)
        k_pos = start - WINDOW + jnp.arange(span, dtype=jnp.int32)
        allowed = (jnp.abs(k_pos[None, :] - q_pos[:, None]) <= WINDOW) & (k_pos >= 0)[None, :] & (k_pos < seq_len)[None, :]
        return attend_block(block_q, block_k, block_v, allowed, ctx_keys, ctx_values, sink)
    attn = lax.map(one_block, jnp.arange(N_SP, dtype=jnp.int32)).reshape(seq_len, samples_n, HEADS * HEAD_DIM)
    group_width = HEADS * HEAD_DIM // N_TP
    branch = jnp.zeros((seq_len, samples_n, D), jnp.float32)
    for group in range(N_TP):
        part = jnp.dot(attn[..., group * group_width:(group + 1) * group_width], w_out[group * group_width:(group + 1) * group_width], preferred_element_type=jnp.float32)
        branch = branch + part.astype(jnp.bfloat16).astype(jnp.float32)
    return (latent.astype(jnp.float32) + gate[None] * branch).astype(jnp.bfloat16)
```

```python
import functools

import jax
import jax.numpy as jnp
from jax import lax
from jax.experimental import pallas as pl
from jax.experimental.pallas import tpu as pltpu
from jax.sharding import PartitionSpec as P

HEAD_DIM = 128
WINDOW = 128
GRID_W = 64
EPSILON = 1e-06
NEGATIVE = -1e30
LOG2E = 1.4426950408889634

SLOT_REL = (0, 1, 3, 2)
REL_SLOT = (0, 1, 3, 2)

bf16 = jnp.bfloat16
f32 = jnp.float32
VMEM = pltpu.VMEM


def cost(flops, size, exps=0):
    return pl.CostEstimate(flops=int(flops), bytes_accessed=int(size), transcendentals=int(exps))


def shifted(array, step, axis):
    size = lax.axis_size(axis)
    return lax.ppermute(array, axis, [(i, (i + step) % size) for i in range(size)])


def sent_to_all(shard, axis):
    length = lax.axis_size(axis)
    return lax.all_to_all(
        jnp.broadcast_to(shard[None], (length, *shard.shape)), axis, 0, 0, tiled=True
    )


def modulation_kernel(cond_ref, ctx_ref, shift_ref, scale_ref, gate_ref, out_ref, both):
    both[...] = jnp.zeros_like(both)
    both[0:2, :] = cond_ref[...].astype(f32)
    both[2:3, :] = ctx_ref[...].astype(f32)
    raw = both[...]
    act = (raw / (1.0 + jnp.exp(-raw))).astype(bf16)
    out_ref[0:3, :] = jnp.dot(act, shift_ref[...], preferred_element_type=f32)[0:3]
    out_ref[3:6, :] = jnp.dot(act, scale_ref[...], preferred_element_type=f32)[0:3]
    out_ref[6:8, :] = jnp.dot(act, gate_ref[...], preferred_element_type=f32)[0:2]


def modulation(condition, ctx_condition, w_shift, w_scale, w_gate):
    depth, width = w_shift.shape
    return pl.pallas_call(
        modulation_kernel,
        out_shape=jax.ShapeDtypeStruct((8, width), f32),
        scratch_shapes=[VMEM((8, depth), f32)],
        cost_estimate=cost(6e6, 3 * depth * width * 2),
        name="modulation",
    )(condition, ctx_condition[None], w_shift, w_scale, w_gate)


def modulated_into(h_ref, row, x_ref, where, rows, gain, shift):
    step = 16

    @pl.loop(0, rows // step)
    def _(i):
        at = pl.multiple_of(i * step, step)
        x = x_ref[(*where, pl.ds(at, step), slice(None))].astype(f32)
        mean = jnp.mean(x * x, axis=-1, keepdims=True)
        h = x * lax.rsqrt(mean + EPSILON) * gain + shift
        h_ref[pl.ds(row + at, step), :] = h.astype(bf16)


def turned(u, cosine, sine):
    lane = lax.broadcasted_iota(jnp.int32, u.shape, 1)
    swapped = jnp.where(lane % 64 < 32, pltpu.roll(u, 96, 1), pltpu.roll(u, 32, 1))
    return u * cosine + swapped * sine


def project_kernel(pieces, tokens, *refs):
    count = len(pieces)
    x_refs = refs[:count]
    gain_ref, mod_ref, cos_ref, sin_ref, wq_ref, wkv_ref, q_ref, kv_ref, h_ref = refs[count:]
    total = 2 * tokens
    for x_ref, (sample, first, rows, where) in zip(x_refs, pieces):
        for at, b in enumerate(sample):
            gain = gain_ref[...] * (1.0 + mod_ref[3 + b : 4 + b, :])
            shift = mod_ref[b : b + 1, :]
            modulated_into(
                h_ref, b * tokens + first, x_ref, (at,) if where else (), rows, gain, shift
            )
    step = 256

    @pl.loop(0, total // step)
    def _(i):
        at = pl.multiple_of(i * step, step)
        h = h_ref[pl.ds(at, step), :]
        qs = jnp.dot(h, wq_ref[...], preferred_element_type=f32)
        kvs = jnp.dot(h, wkv_ref[...], preferred_element_type=f32)
        for part in range(step // 128):
            row = at + part * 128
            b = row // tokens
            tok = pl.multiple_of(row % tokens, 128)
            cosine = cos_ref[pl.ds(tok, 128), :]
            sine = sin_ref[pl.ds(tok, 128), :]
            rows = slice(part * 128, part * 128 + 128)
            for n in range(4):
                u = turned(qs[rows, n * 128 : n * 128 + 128], cosine, sine)
                q_ref[b, n, pl.ds(tok, 128), :] = u.astype(bf16)
            u = turned(kvs[rows, :128], cosine, sine)
            kv_ref[b, 0, pl.ds(tok, 128), :] = u.astype(bf16)
            kv_ref[b, 1, pl.ds(tok, 128), :] = kvs[rows, 128:].astype(bf16)


def project(arrays, pieces, tokens, gain, mod, cosine, sine, w_query, w_kv, name):
    width = gain.shape[1]
    return pl.pallas_call(
        functools.partial(project_kernel, pieces, tokens),
        out_shape=(
            jax.ShapeDtypeStruct((2, 4, tokens, HEAD_DIM), bf16),
            jax.ShapeDtypeStruct((2, 2, tokens, HEAD_DIM), bf16),
        ),
        scratch_shapes=[VMEM((2 * tokens, width), bf16)],
        cost_estimate=cost(2 * 2 * tokens * width * 768, 2 * tokens * width * 2 + width * 768 * 2),
        name=name,
    )(*arrays, gain, mod, cosine, sine, w_query, w_kv)


def context_kernel(x_ref, gain_ref, mod_ref, wkv_ref, out_ref, h_ref):
    rows = x_ref.shape[1]
    gain = gain_ref[...] * (1.0 + mod_ref[5:6, :])
    shift = mod_ref[2:3, :]
    for b in range(2):
        modulated_into(h_ref, b * rows, x_ref, (b,), rows, gain, shift)
    kv = jnp.dot(h_ref[...], wkv_ref[...], preferred_element_type=f32).astype(bf16)
    for b in range(2):
        out_ref[b] = kv[b * rows : (b + 1) * rows]


def project_context(context, gain, mod, w_kv):
    samples, rows, width = context.shape
    return pl.pallas_call(
        context_kernel,
        out_shape=jax.ShapeDtypeStruct((samples, rows, w_kv.shape[1]), bf16),
        scratch_shapes=[VMEM((samples * rows, width), bf16)],
        cost_estimate=cost(2 * 2 * rows * width * 256, 2 * rows * width * 2 + width * 512),
        name="project_context",
    )(context, gain, mod, w_kv)


def attention_kernel(
    table_ref, sink_ref, qa_ref, qb_ref, kva_ref, kvb_ref, before_ref, after_ref,
    ctx_ref, out_ref, keys, values, tiles,
):
    slot = pl.program_id(1)
    ctx_len = ctx_ref.shape[0] * ctx_ref.shape[2]

    @pl.when(slot == 0)
    def _():
        pair = ctx_ref[:, 0].reshape(ctx_len, 2 * HEAD_DIM)
        keys[0:ctx_len, :] = pair[:, :HEAD_DIM]
        values[0:ctx_len, :] = pair[:, HEAD_DIM:]
        for which in range(2):
            tiles[which, 0:384, :] = kva_ref[0, which]
            tiles[which, 384:512, :] = kvb_ref[0, which]
            tiles[which, 512:640, :] = before_ref[0, which]
            tiles[which, 640:768, :] = after_ref[0, which]

    prev = pl.multiple_of(table_ref[slot, 0] * 128, 128)
    here = pl.multiple_of(slot * 128, 128)
    after = pl.multiple_of(table_ref[slot, 1] * 128, 128)
    for to, start in enumerate((prev, here, after)):
        rows = slice(ctx_len + to * 128, ctx_len + to * 128 + 128)
        keys[rows, :] = tiles[0, pl.ds(start, 128), :]
        values[rows, :] = tiles[1, pl.ds(start, 128), :]
    ahead = lax.broadcasted_iota(jnp.int32, (128, 128), 1) - lax.broadcasted_iota(
        jnp.int32, (128, 128), 0
    )
    keep_prev = ahead >= table_ref[slot, 2]
    keep_after = ahead <= -table_ref[slot, 3]
    factor = HEAD_DIM ** (-0.5) * LOG2E
    last = slot == 3
    for n in range(4):
        q = jnp.where(last, qb_ref[0, n], qa_ref[0, n])
        scores = lax.dot_general(
            q, keys[...], (((1,), (1,)), ((), ())), preferred_element_type=f32
        )
        parts = [
            scores[:, : ctx_len],
            jnp.where(keep_prev, scores[:, ctx_len : ctx_len + 128], NEGATIVE),
            scores[:, ctx_len + 128 : ctx_len + 256],
            jnp.where(keep_after, scores[:, ctx_len + 256 :], NEGATIVE),
        ]
        sink = sink_ref[n] * LOG2E
        top = functools.reduce(
            jnp.maximum, [jnp.max(part, axis=-1, keepdims=True) for part in parts]
        )
        top = jnp.maximum(top * factor, sink)
        weights = [jnp.exp2(part * factor - top) for part in parts]
        total = sum(jnp.sum(w, axis=-1, keepdims=True) for w in weights) + jnp.exp2(sink - top)
        weights = jnp.concatenate([w.astype(bf16) for w in weights], axis=1)
        result = jnp.dot(weights, values[...], preferred_element_type=f32) / total
        out_ref[0, 0, :, n * 128 : n * 128 + 128] = result.astype(bf16)


def attention(table, sink, q_a, q_b, kv_a, kv_b, before, after, ctx):
    parts, _, rows, _ = ctx.shape
    ctx_len = parts * rows
    span = ctx_len + 3 * 128
    work = 8 * 4 * 128 * span
    grid_spec = pltpu.PrefetchScalarGridSpec(
        num_scalar_prefetch=2,
        grid=(2, 4),
        in_specs=[
            pl.BlockSpec((1, 4, 128, HEAD_DIM), lambda b, r, *_: (b, 0, jnp.minimum(r, 2), 0)),
            pl.BlockSpec((1, 4, 128, HEAD_DIM), lambda b, r, *_: (b, 0, 0, 0)),
            pl.BlockSpec((1, 2, 384, HEAD_DIM), lambda b, r, *_: (b, 0, 0, 0)),
            pl.BlockSpec((1, 2, 128, HEAD_DIM), lambda b, r, *_: (b, 0, 0, 0)),
            pl.BlockSpec((1, 2, 128, HEAD_DIM), lambda b, r, *_: (b, 0, 0, 0)),
            pl.BlockSpec((1, 2, 128, HEAD_DIM), lambda b, r, *_: (b, 0, 0, 0)),
            pl.BlockSpec((parts, 1, rows, 2 * HEAD_DIM), lambda b, r, *_: (0, b, 0, 0)),
        ],
        out_specs=pl.BlockSpec((1, 1, 128, 512), lambda b, r, *_: (r, b, 0, 0)),
        scratch_shapes=[
            VMEM((span, HEAD_DIM), bf16),
            VMEM((span, HEAD_DIM), bf16),
            VMEM((2, 768, HEAD_DIM), bf16),
        ],
    )
    return pl.pallas_call(
        attention_kernel,
        grid_spec=grid_spec,
        out_shape=jax.ShapeDtypeStruct((4, 2, 128, 512), bf16),
        cost_estimate=cost(work * 512, 6e6, work),
        name="attention",
    )(table, sink, q_a, q_b, kv_a, kv_b, before, after, ctx)


def output_kernel(
    half_ref, a0_ref, a1_ref, a2_ref, a3_ref, w0_ref, near_ref, far_ref, mod_ref, lat_ref, out_ref
):
    width = out_ref.shape[2]
    low = half_ref[0] == 0
    part = jnp.dot(a0_ref[...].reshape(256, 512), w0_ref[...], preferred_element_type=f32)
    branch = part.astype(bf16).astype(f32)
    for j, a_ref in enumerate((a1_ref, a2_ref, a3_ref)):
        a = a_ref[...].reshape(256, 512)
        a_near = jnp.where(low, a[:, :256], a[:, 256:])
        a_far = jnp.where(low, a[:, 256:], a[:, :256])
        part = jnp.dot(
            a_near, near_ref[:, j].reshape(256, width), preferred_element_type=f32
        ) + jnp.dot(a_far, far_ref[:, j].reshape(256, width), preferred_element_type=f32)
        branch = branch + part.astype(bf16).astype(f32)
    for b in range(2):
        gate = mod_ref[6 + b : 7 + b, :]
        mixed = lat_ref[b].astype(f32) + gate * branch[b * 128 : b * 128 + 128]
        out_ref[b] = mixed.astype(bf16)


def output(half, attn, w_own, w_near, w_far, mod, latent):
    samples, rows, width = latent.shape
    tile = 512
    small = pl.BlockSpec((2, 128, 512), lambda n, *_: (0, 0, 0))
    gathered = pl.BlockSpec((16, 3, 16, tile), lambda n, *_: (0, 0, 0, n))
    grid_spec = pltpu.PrefetchScalarGridSpec(
        num_scalar_prefetch=1,
        grid=(width // tile,),
        in_specs=[
            small, small, small, small,
            pl.BlockSpec((512, tile), lambda n, *_: (0, n)),
            gathered, gathered,
            pl.BlockSpec((8, tile), lambda n, *_: (0, n)),
            pl.BlockSpec((samples, rows, tile), lambda n, *_: (0, 0, n)),
        ],
        out_specs=pl.BlockSpec((samples, rows, tile), lambda n, *_: (0, 0, n)),
    )
    return pl.pallas_call(
        output_kernel,
        grid_spec=grid_spec,
        out_shape=jax.ShapeDtypeStruct(latent.shape, bf16),
        cost_estimate=cost(2 * 256 * width * width, width * width * 2 + 4e6),
        name="output",
    )(half, *attn, w_own, w_near, w_far, mod, latent)


def rotation_tables(position):
    quarter = HEAD_DIM // 4
    freqs = 10000.0 ** (-jnp.arange(quarter, dtype=f32) / quarter)
    row = (position // GRID_W).astype(f32)[:, None] * freqs
    col = (position % GRID_W).astype(f32)[:, None] * freqs
    cosine = jnp.concatenate([jnp.cos(row)] * 2 + [jnp.cos(col)] * 2, axis=1)
    sr, sc = jnp.sin(row), jnp.sin(col)
    return cosine, jnp.concatenate([-sr, sr, -sc, sc], axis=1)


def local(
    latent, context, condition, ctx_condition, norm_gain, w_shift, w_scale, w_gate,
    w_query, w_key, w_value, w_out, sink,
):
    sp, tp, dp = (lax.axis_index(name) for name in ("sp", "tp", "dp"))
    n_sp, n_tp = lax.axis_size("sp"), lax.axis_size("tp")
    rows, _, width = latent.shape

    own = jnp.moveaxis(latent, 1, 0)
    below = shifted(own, 1, "tp")
    above = shifted(own, -1, "tp")
    across_0 = shifted(below[0], 1, "tp")
    across_1 = shifted(above[1], -1, "tp")

    partial = modulation(condition, ctx_condition, w_shift, w_scale, w_gate)
    quarter = sent_to_all(partial, "sp").sum(axis=0)
    around = [quarter] + [shifted(quarter, -j, "tp") for j in (1, 2, 3)]
    twice = jnp.concatenate(around + around[:3], axis=1)
    mod = lax.dynamic_slice_in_dim(
        twice, (n_tp - tp) % n_tp * quarter.shape[1], width, axis=1
    )

    gain = norm_gain[None]
    w_kv = jnp.concatenate([w_key, w_value], axis=1)
    ctx = sent_to_all(project_context(jnp.moveaxis(context, 1, 0), gain, mod, w_kv), "sp")

    share = 256 // n_sp
    mine = lax.dynamic_slice_in_dim(w_out, dp * 256 + sp * share, share, axis=0)
    foreign = jnp.stack([shifted(mine, j, "tp") for j in (1, 2, 3)])
    w_near = sent_to_all(foreign, "sp")
    w_far = shifted(w_near, 1, "dp")

    token = jnp.arange(rows, dtype=jnp.int32)
    chunk = (tp + jnp.array(SLOT_REL, jnp.int32)) % n_tp
    position = ((sp * n_tp + chunk)[:, None] * rows + token[None]).reshape(-1)
    cosine, sine = rotation_tables(position)
    both = (0, 1)
    q_a, kv_a = project(
        (own, above, below),
        tuple((both, at * rows, rows, True) for at in range(3)),
        3 * rows, gain, mod, cosine[: 3 * rows], sine[: 3 * rows], w_query, w_kv, "project_a",
    )
    q_b, kv_b = project(
        (across_0, across_1),
        (((0,), 0, rows, False), ((1,), 0, rows, False)),
        rows, gain, mod, cosine[3 * rows :], sine[3 * rows :], w_query, w_kv, "project_b",
    )

    slots = jnp.array(REL_SLOT, jnp.int32)
    kv_all = jnp.concatenate([kv_a, kv_b], axis=2)

    def chunk_kv(c):
        return lax.dynamic_slice_in_dim(kv_all, slots[(c - tp) % n_tp] * rows, rows, axis=2)

    up = [(i, i + 1) for i in range(n_sp - 1)]
    before = lax.ppermute(chunk_kv(n_tp - 1), "sp", up)
    after = lax.ppermute(chunk_kv(0), "sp", [(j, i) for i, j in up])

    first, last = chunk == 0, chunk == n_tp - 1
    table = jnp.stack(
        [
            jnp.where(first, 4, jnp.array((2, 0, 3, 1), jnp.int32)),
            jnp.where(last, 5, jnp.array((1, 3, 0, 2), jnp.int32)),
            jnp.where(first & (sp == 0), 1000, 0),
            jnp.where(last & (sp == n_sp - 1), 1000, 0),
        ],
        axis=1,
    ).astype(jnp.int32)
    attn = attention(table, sink, q_a, q_b, kv_a, kv_b, before, after, ctx)
    heads = [attn[0]] + [shifted(attn[REL_SLOT[j]], j, "tp") for j in (1, 2, 3)]
    half = jnp.full((1,), dp, jnp.int32)
    mixed = output(half, heads, w_out, w_near, w_far, mod, own)
    return jnp.moveaxis(mixed, 0, 1)


def solution(mesh):
    return jax.shard_map(
        local,
        mesh=mesh,
        in_specs=(
            P(("sp", "tp"), "dp", None),
            P("sp", "dp", None),
            P("dp", "sp"),
            P("sp"),
            P(),
            P("sp", "tp"),
            P("sp", "tp"),
            P("sp", "tp"),
            P(None, "tp"),
            P(None, "tp"),
            P(None, "tp"),
            P("tp", None),
            P("tp"),
        ),
        out_specs=P(("sp", "tp"), "dp", None),
        check_vma=False,
    )
```

```python
import functools

import jax
import jax.numpy as jnp
import numpy as np
from jax import lax
from jax.experimental import pallas as pl
from jax.experimental.pallas import tpu as pltpu
from jax.sharding import PartitionSpec as P


HEAD_DIM = 128
GRID_W = 64
SEQ = 8192
EPSILON = 1e-06
NEGATIVE = -1e30
LOG2E = 1.4426950408889634

SLOT_REL = (0, 1, 3, 2)
REL_SLOT = (0, 1, 3, 2)

bf16 = jnp.bfloat16
f32 = jnp.float32
VMEM = pltpu.VMEM


def cost(flops, size, exps=0):
    return pl.CostEstimate(flops=int(flops), bytes_accessed=int(size), transcendentals=int(exps))


def shifted(array, step, axis):
    size = lax.axis_size(axis)
    return lax.ppermute(array, axis, [(i, (i + step) % size) for i in range(size)])


def modulation_kernel(cond_ref, ctx_ref, shift_ref, scale_ref, gate_ref, out_ref, both, rows):
    both[...] = jnp.zeros_like(both)
    both[0:2, :] = cond_ref[...].astype(f32)
    both[2:3, :] = ctx_ref[...].astype(f32)
    raw = both[...]
    act = (raw / (1.0 + jnp.exp(-raw))).astype(bf16)
    rows[0:3, :] = jnp.dot(act, shift_ref[...], preferred_element_type=f32)[0:3]
    rows[3:6, :] = jnp.dot(act, scale_ref[...], preferred_element_type=f32)[0:3]
    rows[6:8, :] = jnp.dot(act, gate_ref[...], preferred_element_type=f32)[0:2]
    for copy in range(out_ref.shape[0]):
        out_ref[copy] = rows[...]


def modulation(copies, condition, ctx_condition, w_shift, w_scale, w_gate):
    depth, width = w_shift.shape
    return pl.pallas_call(
        modulation_kernel,
        out_shape=jax.ShapeDtypeStruct((copies, 8, width), f32),
        scratch_shapes=[VMEM((8, depth), f32), VMEM((8, width), f32)],
        cost_estimate=cost(6e6, 3 * depth * width * 2),
        name="modulation",
    )(condition, ctx_condition[None], w_shift, w_scale, w_gate)


def modulated_into(h_ref, row, x_ref, where, rows, gain, shift):
    step = 64
    for at in range(0, rows, step):
        x = x_ref[(*where, slice(at, at + step), slice(None))].astype(f32)
        mean = jnp.mean(x * x, axis=-1, keepdims=True)
        h = x * lax.rsqrt(mean + EPSILON) * gain + shift
        h_ref[row + at : row + at + step, :] = h.astype(bf16)


def turned(u, cosine, sine):
    lane = lax.broadcasted_iota(jnp.int32, u.shape, 1)
    swapped = jnp.where(lane % 64 < 32, pltpu.roll(u, 96, 1), pltpu.roll(u, 32, 1))
    return u * cosine + swapped * sine


def project_kernel(*refs):
    x_refs, refs = refs[:8], refs[8:]
    where_ref, gain_ref, mod_ref, row_cos, row_sin, col_cos, col_sin = refs[:7]
    wq_ref, wk_ref, wv_ref, q_ref, kv_ref, up_ref, down_ref, x_all, h_ref, w_all, sems = refs[7:]
    sp, tp = where_ref[0], where_ref[1]
    copies = [
        pltpu.make_async_copy(x_ref, x_all.at[i], sems.at[i]) for i, x_ref in enumerate(x_refs)
    ]
    weights = [
        pltpu.make_async_copy(wq_ref, w_all.at[:, 0:512], sems.at[8]),
        pltpu.make_async_copy(wk_ref, w_all.at[:, 512:640], sems.at[9]),
        pltpu.make_async_copy(wv_ref, w_all.at[:, 640:768], sems.at[10]),
    ]
    for copy in copies[:2] + weights + copies[2:]:
        copy.start()
    gains = [gain_ref[...] * (1.0 + mod_ref[3 + b : 4 + b, :]) for b in range(2)]
    left = lax.broadcasted_iota(jnp.int32, (GRID_W, HEAD_DIM), 1) < HEAD_DIM // 2

    def prepare(c):
        for b in range(2):
            copies[2 * c + b].wait()
            shift = mod_ref[b : b + 1, :]
            modulated_into(h_ref.at[c], b * 128, x_all, (2 * c + b,), 128, gains[b], shift)

    def table(row_ref, col_ref, row):
        parts = [
            jnp.where(left, row_ref[pl.ds(row + i, 1), :], col_ref[...]) for i in range(2)
        ]
        return jnp.concatenate(parts, axis=0)

    for c in range(4):
        prepare(c)
    for copy in weights:
        copy.wait()
    chunks = [lax.rem(tp + SLOT_REL[c], 4) for c in range(4)]
    tables = []
    for c in range(4):
        row = sp * 8 + chunks[c] * 2
        tables.append((table(row_cos, col_cos, row), table(row_sin, col_sin, row)))
    for n in range(3):
        product = jnp.dot(
            h_ref[...].reshape(1024, h_ref.shape[2]),
            w_all[:, n * 256 : n * 256 + 256],
            preferred_element_type=f32,
        )
        for c in range(4):
            tok = slice(c * 128, c * 128 + 128)
            for b in range(2):
                rows = slice(c * 256 + b * 128, c * 256 + b * 128 + 128)
                left_part = turned(product[rows, :128], *tables[c]).astype(bf16)
                if n < 2:
                    right_part = turned(product[rows, 128:], *tables[c]).astype(bf16)
                    q_ref[b, 2 * n, tok, :] = left_part
                    q_ref[b, 2 * n + 1, tok, :] = right_part
                else:
                    right_part = product[rows, 128:].astype(bf16)
                    kv_ref[b, 0, tok, :] = left_part
                    kv_ref[b, 1, tok, :] = right_part
    for c in range(4):
        tok = slice(c * 128, c * 128 + 128)
        for to_ref, edge in ((up_ref, 3), (down_ref, 0)):

            @pl.when(chunks[c] == edge)
            def _():
                to_ref[...] = kv_ref[:, :, tok, :]


def project(arrays, where, gain, mod, weights):
    width = gain.shape[1]
    anywhere = pl.BlockSpec(memory_space=pl.ANY)
    whole = pl.BlockSpec(memory_space=VMEM)
    scalars = pl.BlockSpec(memory_space=pltpu.SMEM)
    shapes = [(2, 4, 512, HEAD_DIM), (2, 2, 512, HEAD_DIM)] + [(2, 2, 128, HEAD_DIM)] * 2
    return pl.pallas_call(
        project_kernel,
        in_specs=[anywhere] * 8 + [scalars] + [whole] * 6 + [anywhere] * 3,
        out_specs=tuple(whole for _ in shapes),
        out_shape=tuple(jax.ShapeDtypeStruct(shape, bf16) for shape in shapes),
        scratch_shapes=[
            VMEM((8, 128, width), bf16),
            VMEM((4, 256, width), bf16),
            VMEM((width, 768), bf16),
            pltpu.SemaphoreType.DMA((11,)),
        ],
        cost_estimate=cost(2 * 1024 * width * 768, 8e6),
        name="project",
    )(*arrays, where, gain, mod, *rotation_tables(), *weights)


def context_kernel(x_ref, gain_ref, mod_ref, wk_ref, wv_ref, out_ref, h_ref):
    rows = x_ref.shape[1]
    gain = gain_ref[...] * (1.0 + mod_ref[5:6, :])
    shift = mod_ref[2:3, :]
    for b in range(2):
        modulated_into(h_ref, b * rows, x_ref, (b,), rows, gain, shift)
    for which, w_ref in enumerate((wk_ref, wv_ref)):
        part = jnp.dot(h_ref[...], w_ref[...], preferred_element_type=f32).astype(bf16)
        for copy in range(out_ref.shape[0]):
            for b in range(2):
                out_ref[copy, b, :, which * 128 : which * 128 + 128] = part[
                    b * rows : (b + 1) * rows
                ]


def project_context(copies, context, gain, mod, w_key, w_value):
    samples, rows, width = context.shape
    return pl.pallas_call(
        context_kernel,
        out_shape=jax.ShapeDtypeStruct((copies, samples, rows, 2 * HEAD_DIM), bf16),
        scratch_shapes=[VMEM((samples * rows, width), bf16)],
        cost_estimate=cost(2 * 2 * rows * width * 256, 2 * rows * width * 2 + width * 512),
        name="project_context",
    )(context, gain, mod, w_key, w_value)


def attention_kernel(
    where_ref, sink_ref, q_ref, kv_ref, before_ref, after_ref, ctx_ref,
    out0, out1, out2, out3, ctx_k, ctx_v, tile_k, tile_v, near_k, near_v,
):
    ctx_len = ctx_k.shape[0]
    pair = ctx_ref[:, 0].reshape(ctx_len, 2 * HEAD_DIM)
    ctx_k[...] = pair[:, :HEAD_DIM]
    ctx_v[:, :HEAD_DIM] = pair[:, HEAD_DIM:]
    ctx_v[:, HEAD_DIM:] = jnp.ones((ctx_len, HEAD_DIM), bf16)
    near_v[:, :, HEAD_DIM:] = jnp.ones((4, 384, HEAD_DIM), bf16)
    for tile, which in ((tile_k, 0), (tile_v, 1)):
        tile[0:512, :] = kv_ref[0, which]
        tile[512:640, :] = before_ref[0, which]
        tile[640:768, :] = after_ref[0, which]
    sp, tp = where_ref[0], where_ref[1]
    chunks = [lax.rem(tp + SLOT_REL[slot], 4) for slot in range(4)]
    for slot in range(4):
        prev = jnp.where(chunks[slot] == 0, 4, REL_SLOT[(SLOT_REL[slot] + 3) % 4])
        after = jnp.where(chunks[slot] == 3, 5, REL_SLOT[(SLOT_REL[slot] + 1) % 4])
        prev = pl.multiple_of(prev * 128, 128)
        after = pl.multiple_of(after * 128, 128)
        for to, start in enumerate((prev, slot * 128, after)):
            rows = slice(to * 128, to * 128 + 128)
            near_k[slot, rows, :] = tile_k[pl.ds(start, 128), :]
            near_v[slot, rows, :HEAD_DIM] = tile_v[pl.ds(start, 128), :]
    ahead = lax.broadcasted_iota(jnp.int32, (128, 128), 1) - lax.broadcasted_iota(
        jnp.int32, (128, 128), 0
    )
    factor = HEAD_DIM ** (-0.5) * LOG2E
    across = (((1,), (1,)), ((), ()))
    for slot, out_ref in enumerate((out0, out1, out2, out3)):
        q = q_ref[0, :, slot * 128 : slot * 128 + 128, :].reshape(512, HEAD_DIM)
        far = lax.dot_general(q, ctx_k[...], across, preferred_element_type=f32)
        near = lax.dot_general(q, near_k[slot], across, preferred_element_type=f32)
        no_prev = (chunks[slot] == 0) & (sp == 0)
        no_after = (chunks[slot] == 3) & (sp == SEQ // 512 - 1)
        keep_prev = ahead >= jnp.where(no_prev, 1000, 0)
        keep_after = ahead <= jnp.where(no_after, -1000, 0)
        far_weights, near_weights, sinks = [], [], []
        for n in range(4):
            rows = slice(n * 128, n * 128 + 128)
            parts = [
                far[rows],
                jnp.where(keep_prev, near[rows, :128], NEGATIVE),
                near[rows, 128:256],
                jnp.where(keep_after, near[rows, 256:], NEGATIVE),
            ]
            sink = sink_ref[n] * LOG2E
            top = functools.reduce(
                jnp.maximum, [jnp.max(part, axis=-1, keepdims=True) for part in parts]
            )
            top = jnp.maximum(top * factor, sink)
            weights = [jnp.exp2(part * factor - top).astype(bf16) for part in parts]
            far_weights.append(weights[0])
            near_weights.append(jnp.concatenate(weights[1:], axis=1))
            sinks.append(jnp.exp2(sink - top))
        both = jnp.dot(
            jnp.concatenate(far_weights, axis=0), ctx_v[...], preferred_element_type=f32
        ) + jnp.dot(
            jnp.concatenate(near_weights, axis=0), near_v[slot], preferred_element_type=f32
        )
        for n in range(4):
            rows = slice(n * 128, n * 128 + 128)
            total = both[rows, HEAD_DIM:] + sinks[n]
            out_ref[:, rows] = (both[rows, :HEAD_DIM] / total).astype(bf16)


def attention(b, where, sink, q, kv, before, after, ctx):
    parts, _, rows, _ = ctx.shape
    ctx_len = parts * rows
    work = 4 * 4 * 128 * (ctx_len + 384)
    out = pl.BlockSpec((128, 512), lambda i, *_: (0, 0))
    edge = pl.BlockSpec((1, 2, 128, HEAD_DIM), lambda i, *_: (b, 0, 0, 0))
    grid_spec = pltpu.PrefetchScalarGridSpec(
        num_scalar_prefetch=2,
        grid=(1,),
        in_specs=[
            pl.BlockSpec((1, 4, 512, HEAD_DIM), lambda i, *_: (b, 0, 0, 0)),
            pl.BlockSpec((1, 2, 512, HEAD_DIM), lambda i, *_: (b, 0, 0, 0)),
            edge, edge,
            pl.BlockSpec((parts, 1, rows, 2 * HEAD_DIM), lambda i, *_: (0, b, 0, 0)),
        ],
        out_specs=(out,) * 4,
        scratch_shapes=[
            VMEM((ctx_len, HEAD_DIM), bf16),
            VMEM((ctx_len, 2 * HEAD_DIM), bf16),
            VMEM((768, HEAD_DIM), bf16),
            VMEM((768, HEAD_DIM), bf16),
            VMEM((4, 384, HEAD_DIM), bf16),
            VMEM((4, 384, 2 * HEAD_DIM), bf16),
        ],
    )
    return pl.pallas_call(
        attention_kernel,
        grid_spec=grid_spec,
        out_shape=(jax.ShapeDtypeStruct((128, 512), bf16),) * 4,
        cost_estimate=cost(work * 512, 3e6, work),
    )(where, sink, q, kv, before, after, ctx)


def own_heads_kernel(a0_ref, a1_ref, w0_ref, branch_ref):
    heads = jnp.concatenate([a0_ref[...], a1_ref[...]], axis=0)
    part = jnp.dot(heads, w0_ref[...], preferred_element_type=f32)
    branch_ref[...] = part.astype(bf16)


def own_heads(attn, w_own):
    depth, width = w_own.shape
    tile = 1024
    whole = pl.BlockSpec((128, 512), lambda n: (0, 0))
    return pl.pallas_call(
        own_heads_kernel,
        grid=(width // tile,),
        in_specs=[whole] * 2 + [pl.BlockSpec((depth, tile), lambda n: (0, n))],
        out_specs=pl.BlockSpec((256, tile), lambda n: (0, n)),
        out_shape=jax.ShapeDtypeStruct((256, width), bf16),
        cost_estimate=cost(2 * 256 * depth * width, 3e6),
        name="own_heads",
    )(*attn, w_own)


def output_kernel(where_ref, *refs):
    a_refs, w_refs = refs[:6], refs[6:14]
    branch_ref, mod_ref, lat0_ref, lat1_ref, out_ref = refs[14:]
    low = where_ref[2] == 0
    total = branch_ref[...].astype(f32)
    pieces = (w_refs[0:2], w_refs[2:6], w_refs[6:8])
    for j in range(3):
        a = jnp.concatenate([a_refs[2 * j][...], a_refs[2 * j + 1][...]], axis=0)
        a_near = jnp.where(low, a[:, :256], a[:, 256:])
        a_far = jnp.where(low, a[:, 256:], a[:, :256])
        w = jnp.concatenate([ref[...] for ref in pieces[j]], axis=0)
        part = jnp.dot(
            jnp.concatenate([a_near, a_far], axis=1), w, preferred_element_type=f32
        )
        total = total + part.astype(bf16).astype(f32)
    for b, lat_ref in enumerate((lat0_ref, lat1_ref)):
        gate = mod_ref[6 + b : 7 + b, :]
        mixed = lat_ref[...].astype(f32) + gate * total[b * 128 : b * 128 + 128]
        out_ref[:, b, :] = mixed.astype(bf16)


def output(where, attn, gathered, branch, mod, latents):
    rows, width = latents[0].shape
    tile = 512
    whole = pl.BlockSpec((rows, 512), lambda n: (0, 0))

    def columns(*lead):
        return pl.BlockSpec((*lead, tile), lambda n: (0,) * len(lead) + (n,))

    return pl.pallas_call(
        output_kernel,
        grid=(width // tile,),
        in_specs=[pl.BlockSpec(memory_space=pltpu.SMEM)]
        + [whole] * 6
        + [columns(array.shape[0]) for array in gathered]
        + [columns(256), columns(8), columns(rows), columns(rows)],
        out_specs=columns(rows, 2),
        out_shape=jax.ShapeDtypeStruct((rows, 2, width), bf16),
        cost_estimate=cost(2 * 256 * width * width * 3 // 4, 10e6),
        name="output",
    )(where, *attn, *gathered, branch, mod, *latents)


def rotation_tables():
    quarter = HEAD_DIM // 4
    freqs = np.float32(10000.0) ** (-np.arange(quarter, dtype=np.float32) / np.float32(quarter))
    tables = []
    for count, left in ((SEQ // GRID_W, True), (GRID_W, False)):
        angle = (np.arange(count, dtype=np.float32)[:, None] * freqs).astype(np.float64)
        cosine = np.concatenate([np.cos(angle)] * 2, axis=1)
        sine = np.concatenate([-np.sin(angle), np.sin(angle)], axis=1)
        for values in (cosine, sine):
            pair = [values, np.zeros_like(values)]
            table = np.concatenate(pair if left else pair[::-1], axis=1)
            tables.append(jnp.asarray(table.astype(np.float32)))
    return tables


def block(
    latent, context, condition, ctx_condition, norm_gain, w_shift, w_scale, w_gate,
    w_query, w_key, w_value, w_out, sink,
):
    sp, tp, dp = (lax.axis_index(name) for name in ("sp", "tp", "dp"))
    n_sp, n_tp = lax.axis_size("sp"), lax.axis_size("tp")
    _, _, width = latent.shape

    own = tuple(latent[:, b] for b in range(2))
    below_0 = shifted(own[0], 1, "tp")
    above_1 = shifted(own[1], -1, "tp")
    below_1 = shifted(own[1], 1, "tp")
    above_0 = shifted(own[0], -1, "tp")
    across_0 = shifted(below_0, 1, "tp")
    across_1 = shifted(above_1, -1, "tp")

    partial = modulation(n_sp, condition, ctx_condition, w_shift, w_scale, w_gate)
    quarters = lax.all_to_all(partial, "sp", 0, 0, tiled=True)
    quarter = quarters.sum(axis=0)
    around = [quarter]
    for j in (1, 2, 3):
        around.append(shifted(quarter, -j, "tp"))
    twice = jnp.concatenate(around + around[:3], axis=1)
    mod = lax.dynamic_slice_in_dim(
        twice, (n_tp - tp) % n_tp * quarter.shape[1], width, axis=1
    )

    gain = norm_gain[None]
    ctx = project_context(n_sp, jnp.moveaxis(context, 1, 0), gain, mod, w_key, w_value)
    ctx = lax.all_to_all(ctx, "sp", 0, 0, tiled=True)

    half = lax.dynamic_slice_in_dim(w_out, dp * 256, 256, axis=0)
    w_below = shifted(half, 1, "tp")
    w_above = shifted(half, -1, "tp")
    w_across_0 = shifted(w_below[:128], 1, "tp")
    w_across_1 = shifted(w_above[128:], -1, "tp")
    gathered = []
    for array in (w_below, w_across_0, w_across_1, w_above):
        gathered.append((array, shifted(array, 1, "dp")))
    gathered = (
        *gathered[0],
        gathered[1][0], gathered[2][0], gathered[1][1], gathered[2][1],
        *gathered[3],
    )

    where = jnp.stack([sp, tp, dp]).astype(jnp.int32)
    q, kv, up, down = project(
        (*own, above_0, above_1, below_0, below_1, across_0, across_1),
        where, gain, mod, (w_query, w_key, w_value),
    )

    along = [(i, i + 1) for i in range(n_sp - 1)]
    before = lax.ppermute(up, "sp", along)
    after = lax.ppermute(down, "sp", [(j, i) for i, j in along])

    heads = [[None] * 2 for _ in range(4)]
    for b in range(2):
        attn = attention(b, where, sink, q, kv, before, after, ctx)
        heads[0][b] = attn[0]
        for j in (2, 1, 3):
            heads[j][b] = shifted(attn[REL_SLOT[j]], j, "tp")
    branch = own_heads(heads[0], w_out)
    return output(where, heads[1] + heads[2] + heads[3], gathered, branch, mod, own)


def solution(mesh):
    return jax.shard_map(
        block,
        mesh=mesh,
        in_specs=(
            P(("sp", "tp"), "dp", None),
            P("sp", "dp", None),
            P("dp", "sp"),
            P("sp"),
            P(),
            P("sp", "tp"),
            P("sp", "tp"),
            P("sp", "tp"),
            P(None, "tp"),
            P(None, "tp"),
            P(None, "tp"),
            P("tp", None),
            P("tp"),
        ),
        out_specs=P(("sp", "tp"), "dp", None),
        check_vma=False,
    )
```

```python
import functools

import jax
import jax.numpy as jnp
import numpy as np
from jax import lax
from jax.experimental import pallas as pl
from jax.experimental.pallas import tpu as pltpu
from jax.sharding import PartitionSpec as P


HEAD_DIM = 128
GRID_W = 64
SEQ = 8192
EPSILON = 1e-06
NEGATIVE = -1e30
LOG2E = 1.4426950408889634

SLOT_REL = (0, 1, 3, 2)
REL_SLOT = (0, 1, 3, 2)

bf16 = jnp.bfloat16
f32 = jnp.float32
VMEM = pltpu.VMEM


def cost(flops, size, exps=0):
    return pl.CostEstimate(flops=int(flops), bytes_accessed=int(size), transcendentals=int(exps))


def shifted(array, step, axis):
    size = lax.axis_size(axis)
    return lax.ppermute(array, axis, [(i, (i + step) % size) for i in range(size)])


def modulation_kernel(cond_ref, ctx_ref, shift_ref, scale_ref, gate_ref, out_ref, both, rows):
    both[...] = jnp.zeros_like(both)
    both[0:2, :] = cond_ref[...].astype(f32)
    both[2:3, :] = ctx_ref[...].astype(f32)
    raw = both[...]
    act = (raw / (1.0 + jnp.exp(-raw))).astype(bf16)
    rows[0:3, :] = jnp.dot(act, shift_ref[...], preferred_element_type=f32)[0:3]
    rows[3:6, :] = jnp.dot(act, scale_ref[...], preferred_element_type=f32)[0:3]
    rows[6:8, :] = jnp.dot(act, gate_ref[...], preferred_element_type=f32)[0:2]
    for copy in range(out_ref.shape[0]):
        out_ref[copy] = rows[...]


def modulation(copies, condition, ctx_condition, w_shift, w_scale, w_gate):
    depth, width = w_shift.shape
    return pl.pallas_call(
        modulation_kernel,
        out_shape=jax.ShapeDtypeStruct((copies, 8, width), f32),
        scratch_shapes=[VMEM((8, depth), f32), VMEM((8, width), f32)],
        cost_estimate=cost(6e6, 3 * depth * width * 2),
        name="modulation",
        compiler_params=pltpu.CompilerParams(vmem_limit_bytes=4 << 20),
    )(condition, ctx_condition[None], w_shift, w_scale, w_gate)


def modulated_into(h_ref, row, x_ref, where, rows, gain, shift):
    step = 64
    for at in range(0, rows, step):
        x = x_ref[(*where, slice(at, at + step), slice(None))].astype(f32)
        mean = jnp.mean(x * x, axis=-1, keepdims=True)
        h = x * lax.rsqrt(mean + EPSILON) * gain + shift
        h_ref[row + at : row + at + step, :] = h.astype(bf16)


def turned(u, cosine, sine):
    lane = lax.broadcasted_iota(jnp.int32, u.shape, 1)
    swapped = jnp.where(lane % 64 < 32, pltpu.roll(u, 96, 1), pltpu.roll(u, 32, 1))
    return u * cosine + swapped * sine


def project_kernel(*refs):
    x_refs, refs = refs[:8], refs[8:]
    where_ref, gain_ref, mod_ref, row_cos, row_sin, col_cos, col_sin = refs[:7]
    wq_ref, wk_ref, wv_ref, q_ref, kv_ref, up_ref, down_ref, h_ref, w_kv = refs[7:]
    sp, tp = where_ref[0], where_ref[1]
    gains = [gain_ref[...] * (1.0 + mod_ref[3 + b : 4 + b, :]) for b in range(2)]
    left = lax.broadcasted_iota(jnp.int32, (GRID_W, HEAD_DIM), 1) < HEAD_DIM // 2

    def prepare(c):
        for b in range(2):
            shift = mod_ref[b : b + 1, :]
            modulated_into(h_ref.at[c], b * 128, x_refs[2 * c + b], (), 128, gains[b], shift)

    def table(row_ref, col_ref, row):
        parts = [
            jnp.where(left, row_ref[pl.ds(row + i, 1), :], col_ref[...]) for i in range(2)
        ]
        return jnp.concatenate(parts, axis=0)

    for c in range(4):
        prepare(c)
    w_kv[:, :HEAD_DIM] = wk_ref[...]
    w_kv[:, HEAD_DIM:] = wv_ref[...]
    chunks = [lax.rem(tp + SLOT_REL[c], 4) for c in range(4)]
    tables = []
    for c in range(4):
        row = sp * 8 + chunks[c] * 2
        tables.append((table(row_cos, col_cos, row), table(row_sin, col_sin, row)))
    for n in range(3):
        product = jnp.dot(
            h_ref[...].reshape(1024, h_ref.shape[2]),
            wq_ref[:, n * 256 : n * 256 + 256] if n < 2 else w_kv[...],
            preferred_element_type=f32,
        )
        for c in range(4):
            tok = slice(c * 128, c * 128 + 128)
            for b in range(2):
                rows = slice(c * 256 + b * 128, c * 256 + b * 128 + 128)
                left_part = turned(product[rows, :128], *tables[c]).astype(bf16)
                if n < 2:
                    right_part = turned(product[rows, 128:], *tables[c]).astype(bf16)
                    q_ref[b, 2 * n, tok, :] = left_part
                    q_ref[b, 2 * n + 1, tok, :] = right_part
                else:
                    right_part = product[rows, 128:].astype(bf16)
                    kv_ref[b, 0, tok, :] = left_part
                    kv_ref[b, 1, tok, :] = right_part
    for c in range(4):
        tok = slice(c * 128, c * 128 + 128)
        for to_ref, edge in ((up_ref, 3), (down_ref, 0)):

            @pl.when(chunks[c] == edge)
            def _():
                to_ref[...] = kv_ref[:, :, tok, :]


def project(arrays, where, gain, mod, weights):
    width = gain.shape[1]
    whole = pl.BlockSpec(memory_space=VMEM)
    scalars = pl.BlockSpec(memory_space=pltpu.SMEM)
    shapes = [(2, 4, 512, HEAD_DIM), (2, 2, 512, HEAD_DIM)] + [(2, 2, 128, HEAD_DIM)] * 2
    return pl.pallas_call(
        project_kernel,
        in_specs=[whole] * 8 + [scalars] + [whole] * 9,
        out_specs=tuple(whole for _ in shapes),
        out_shape=tuple(jax.ShapeDtypeStruct(shape, bf16) for shape in shapes),
        scratch_shapes=[
            VMEM((4, 256, width), bf16),
            VMEM((width, 2 * HEAD_DIM), bf16),
        ],
        cost_estimate=cost(2 * 1024 * width * 768, 8e6),
        name="project",
        compiler_params=pltpu.CompilerParams(vmem_limit_bytes=28 << 20),
    )(*arrays, where, gain, mod, *rotation_tables(), *weights)


def context_kernel(
    x_ref, where_ref, gain_ref, m0_ref, m1_ref, m2_ref, m3_ref, wk_ref, wv_ref,
    out_ref, mod_ref, h_ref,
):
    rows = x_ref.shape[1]
    quarter = m0_ref.shape[1]
    for j, m_ref in enumerate((m0_ref, m1_ref, m2_ref, m3_ref)):
        at = pl.multiple_of(lax.rem(where_ref[1] + j, 4) * quarter, quarter)
        mod_ref[:, pl.ds(at, quarter)] = m_ref[...]
    gain = gain_ref[...] * (1.0 + mod_ref[5:6, :])
    shift = mod_ref[2:3, :]
    for b in range(2):
        modulated_into(h_ref, b * rows, x_ref, (b,), rows, gain, shift)
    for which, w_ref in enumerate((wk_ref, wv_ref)):
        part = jnp.dot(h_ref[...], w_ref[...], preferred_element_type=f32).astype(bf16)
        for copy in range(out_ref.shape[0]):
            for b in range(2):
                out_ref[copy, b, :, which * 128 : which * 128 + 128] = part[
                    b * rows : (b + 1) * rows
                ]


def project_context(copies, context, where, gain, quarters, w_key, w_value):
    samples, rows, width = context.shape
    return pl.pallas_call(
        context_kernel,
        in_specs=[pl.BlockSpec(memory_space=VMEM), pl.BlockSpec(memory_space=pltpu.SMEM)]
        + [pl.BlockSpec(memory_space=VMEM)] * 7,
        out_shape=(
            jax.ShapeDtypeStruct((copies, samples, rows, 2 * HEAD_DIM), bf16),
            jax.ShapeDtypeStruct((8, width), f32),
        ),
        scratch_shapes=[VMEM((samples * rows, width), bf16)],
        cost_estimate=cost(2 * 2 * rows * width * 256, 2 * rows * width * 2 + width * 512),
        name="project_context",
        compiler_params=pltpu.CompilerParams(vmem_limit_bytes=10 << 20),
    )(context, where, gain, *quarters, w_key, w_value)


def attention_kernel(
    slots, where_ref, sink_ref, q_ref, kv_ref, before_ref, after_ref, ctx_ref, *refs
):
    if slots == (0,):
        w_ref, branch_ref, heads = refs[0], refs[1], refs[-1]
        outs, refs = (heads,), refs[2:-1]
    else:
        outs, refs = refs[: len(slots)], refs[len(slots) :]
    ctx_v, tile_k, tile_v, near_k, near_v = refs
    ctx_len = ctx_v.shape[0]
    sp, tp = where_ref[0], where_ref[1]
    ahead = lax.broadcasted_iota(jnp.int32, (128, 128), 1) - lax.broadcasted_iota(
        jnp.int32, (128, 128), 0
    )
    factor = HEAD_DIM ** (-0.5) * LOG2E
    across = (((1,), (1,)), ((), ()))
    ctx_v[:, HEAD_DIM:] = jnp.ones((ctx_len, HEAD_DIM), bf16)
    near_v[:, :, HEAD_DIM:] = jnp.ones((len(slots), 384, HEAD_DIM), bf16)
    for b in range(2):
        ctx_k = ctx_ref[:, b, :, :HEAD_DIM].reshape(ctx_len, HEAD_DIM)
        ctx_v[:, :HEAD_DIM] = ctx_ref[:, b, :, HEAD_DIM:].reshape(ctx_len, HEAD_DIM)
        for tile, which in ((tile_k, 0), (tile_v, 1)):
            tile[0:512, :] = kv_ref[b, which]
            tile[512:640, :] = before_ref[b, which]
            tile[640:768, :] = after_ref[b, which]
        for at, (slot, out_ref) in enumerate(zip(slots, outs)):
            chunk = lax.rem(tp + SLOT_REL[slot], 4)
            prev = jnp.where(chunk == 0, 4, REL_SLOT[(SLOT_REL[slot] + 3) % 4])
            after = jnp.where(chunk == 3, 5, REL_SLOT[(SLOT_REL[slot] + 1) % 4])
            starts = (pl.multiple_of(prev * 128, 128), slot * 128, pl.multiple_of(after * 128, 128))
            for to, start in enumerate(starts):
                rows = slice(to * 128, to * 128 + 128)
                near_k[at, rows, :] = tile_k[pl.ds(start, 128), :]
                near_v[at, rows, :HEAD_DIM] = tile_v[pl.ds(start, 128), :]
            q = q_ref[b, :, slot * 128 : slot * 128 + 128, :].reshape(512, HEAD_DIM)
            far = lax.dot_general(q, ctx_k, across, preferred_element_type=f32)
            near = lax.dot_general(q, near_k[at], across, preferred_element_type=f32)
            no_prev = (chunk == 0) & (sp == 0)
            no_after = (chunk == 3) & (sp == SEQ // 512 - 1)
            keep_prev = ahead >= jnp.where(no_prev, 1000, 0)
            keep_after = ahead <= jnp.where(no_after, -1000, 0)
            far_weights, near_weights, sinks = [], [], []
            for n in range(4):
                rows = slice(n * 128, n * 128 + 128)
                parts = [
                    far[rows],
                    jnp.where(keep_prev, near[rows, :128], NEGATIVE),
                    near[rows, 128:256],
                    jnp.where(keep_after, near[rows, 256:], NEGATIVE),
                ]
                sink = sink_ref[n] * LOG2E
                top = functools.reduce(
                    jnp.maximum, [jnp.max(part, axis=-1, keepdims=True) for part in parts]
                )
                top = jnp.maximum(top * factor, sink)
                weights = [jnp.exp2(part * factor - top).astype(bf16) for part in parts]
                far_weights.append(weights[0])
                near_weights.append(jnp.concatenate(weights[1:], axis=1))
                sinks.append(jnp.exp2(sink - top))
            both = jnp.dot(
                jnp.concatenate(far_weights, axis=0), ctx_v[...], preferred_element_type=f32
            ) + jnp.dot(
                jnp.concatenate(near_weights, axis=0), near_v[at], preferred_element_type=f32
            )
            for n in range(4):
                rows = slice(n * 128, n * 128 + 128)
                total = both[rows, HEAD_DIM:] + sinks[n]
                out_ref[b * 128 : b * 128 + 128, rows] = (
                    both[rows, :HEAD_DIM] / total
                ).astype(bf16)
    if slots == (0,):
        part = jnp.dot(heads[...], w_ref[...], preferred_element_type=f32)
        branch_ref[...] = part.astype(bf16)


def attention(slots, where, sink, q, kv, before, after, ctx, w_own=None):
    parts, _, rows, _ = ctx.shape
    ctx_len = parts * rows
    work = 2 * len(slots) * 4 * 128 * (ctx_len + 384)
    whole = pl.BlockSpec(memory_space=VMEM)
    scalars = pl.BlockSpec(memory_space=pltpu.SMEM)
    operands = [where, sink, q, kv, before, after, ctx]
    in_specs = [scalars] * 2 + [whole] * 5
    scratch = [
        VMEM((ctx_len, 2 * HEAD_DIM), bf16),
        VMEM((768, HEAD_DIM), bf16),
        VMEM((768, HEAD_DIM), bf16),
        VMEM((len(slots), 384, HEAD_DIM), bf16),
        VMEM((len(slots), 384, 2 * HEAD_DIM), bf16),
    ]
    shapes = [(256, 512)] * len(slots)
    if slots == (0,):
        operands.append(w_own)
        in_specs.append(whole)
        shapes = [(256, w_own.shape[1])]
        scratch.append(VMEM((256, 512), bf16))
    return pl.pallas_call(
        functools.partial(attention_kernel, slots),
        in_specs=in_specs,
        out_specs=tuple(whole for _ in shapes),
        out_shape=tuple(jax.ShapeDtypeStruct(shape, bf16) for shape in shapes),
        scratch_shapes=scratch,
        cost_estimate=cost(work * 512, 4e6, work),
        compiler_params=pltpu.CompilerParams(vmem_limit_bytes=24 << 20),
    )(*operands)


def output_kernel(where_ref, *refs):
    a_refs, w_refs = refs[:3], refs[3:11]
    branch_ref, mod_ref, lat0_ref, lat1_ref, out_ref = refs[11:]
    sp, dp = where_ref[0], where_ref[2]
    odd_x, odd_z = lax.rem(sp, 2), lax.rem(lax.div(sp, 4), 2)
    at_two = []
    for core, odd in ((dp, jnp.where(dp == 0, odd_x, odd_z)), (1 - dp, jnp.where(dp == 0, odd_z, odd_x))):
        at_two += [core * 256 + odd * 128, core * 256 + (1 - odd) * 128]
    groups = (
        (a_refs[0], (2, 6), (dp * 256, 256 - dp * 256)),
        (a_refs[1], (0, 1, 4, 5), at_two),
        (a_refs[2], (3, 7), (dp * 256, 256 - dp * 256)),
    )
    heads = []
    for a_ref, pieces, starts in groups:
        parts = [
            a_ref[:, pl.ds(pl.multiple_of(start, 128), w_refs[i].shape[0])]
            for i, start in zip(pieces, starts)
        ]
        heads.append(jnp.concatenate(parts, axis=1))
    tile = 512
    for n in range(0, out_ref.shape[2], tile):
        cols = slice(n, n + tile)
        total = branch_ref[:, cols].astype(f32)
        for a, (_, pieces, _) in zip(heads, groups):
            w = jnp.concatenate([w_refs[i][:, cols] for i in pieces], axis=0)
            part = jnp.dot(a, w, preferred_element_type=f32)
            total = total + part.astype(bf16).astype(f32)
        for b, lat_ref in enumerate((lat0_ref, lat1_ref)):
            gate = mod_ref[6 + b : 7 + b, cols]
            mixed = lat_ref[:, cols].astype(f32) + gate * total[b * 128 : b * 128 + 128]
            out_ref[:, b, cols] = mixed.astype(bf16)


def output(where, attn, gathered, branch, mod, latents):
    rows, width = latents[0].shape
    whole = pl.BlockSpec(memory_space=VMEM)
    return pl.pallas_call(
        output_kernel,
        in_specs=[pl.BlockSpec(memory_space=pltpu.SMEM)] + [whole] * (len(attn) + len(gathered) + 4),
        out_specs=whole,
        out_shape=jax.ShapeDtypeStruct((rows, 2, width), bf16),
        cost_estimate=cost(2 * 256 * width * width * 3 // 4, 10e6),
        name="output",
        compiler_params=pltpu.CompilerParams(vmem_limit_bytes=22 << 20),
    )(where, *attn, *gathered, branch, mod, *latents)


def rotation_tables():
    quarter = HEAD_DIM // 4
    freqs = np.float32(10000.0) ** (-np.arange(quarter, dtype=np.float32) / np.float32(quarter))
    tables = []
    for count, left in ((SEQ // GRID_W, True), (GRID_W, False)):
        angle = (np.arange(count, dtype=np.float32)[:, None] * freqs).astype(np.float64)
        cosine = np.concatenate([np.cos(angle)] * 2, axis=1)
        sine = np.concatenate([-np.sin(angle), np.sin(angle)], axis=1)
        for values in (cosine, sine):
            pair = [values, np.zeros_like(values)]
            table = np.concatenate(pair if left else pair[::-1], axis=1)
            tables.append(jnp.asarray(table.astype(np.float32)))
    return tables


def block(
    latent, context, condition, ctx_condition, norm_gain, w_shift, w_scale, w_gate,
    w_query, w_key, w_value, w_out, sink,
):
    sp, tp, dp = (lax.axis_index(name) for name in ("sp", "tp", "dp"))
    n_sp = lax.axis_size("sp")
    where = jnp.stack([sp, tp, dp]).astype(jnp.int32)

    own = tuple(latent[:, b] for b in range(2))
    below_0 = shifted(own[0], 1, "tp")
    above_1 = shifted(own[1], -1, "tp")
    below_1 = shifted(own[1], 1, "tp")
    above_0 = shifted(own[0], -1, "tp")
    across_0 = shifted(below_0, 1, "tp")
    across_1 = shifted(above_1, -1, "tp")

    partial = modulation(n_sp, condition, ctx_condition, w_shift, w_scale, w_gate)
    quarters = lax.all_to_all(partial, "sp", 0, 0, tiled=True)
    quarter = quarters.sum(axis=0)
    around = [quarter]
    for j in (1, 2, 3):
        around.append(shifted(quarter, -j, "tp"))
    gain = norm_gain[None]
    ctx, mod = project_context(
        n_sp, jnp.moveaxis(context, 1, 0), where, gain, around, w_key, w_value
    )
    ctx = lax.all_to_all(ctx, "sp", 0, 0, tiled=True)

    half = lax.dynamic_slice_in_dim(w_out, dp * 256, 256, axis=0)
    parity = jnp.where(dp == 0, sp % 2, sp // 4 % 2)
    part = lax.dynamic_slice_in_dim(w_out, dp * 256 + parity * 128, 128, axis=0)
    pairs = []
    for s in range(n_sp):
        for d in range(2):
            pairs.append((s * 2 + d, (s ^ (1 if d == 0 else 4)) * 2 + d))
    mine = shifted(part, 2, "tp")
    theirs = lax.ppermute(mine, ("sp", "dp"), pairs)
    below = shifted(half, 1, "tp")
    above = shifted(half, -1, "tp")
    gathered = [mine, theirs, below, above]
    for array in tuple(gathered):
        gathered.append(shifted(array, 1, "dp"))

    q, kv, up, down = project(
        (*own, above_0, above_1, below_0, below_1, across_0, across_1),
        where, gain, mod, (w_query, w_key, w_value),
    )

    along = [(i, i + 1) for i in range(n_sp - 1)]
    before = lax.ppermute(up, "sp", along)
    after = lax.ppermute(down, "sp", [(j, i) for i, j in along])

    attn = attention((3, 1, 2), where, sink, q, kv, before, after, ctx)
    heads = []
    for j, array in ((1, attn[1]), (2, attn[0]), (3, attn[2])):
        heads.append(shifted(array, j, "tp"))
    (branch,) = attention((0,), where, sink, q, kv, before, after, ctx, w_out)
    return output(where, heads, gathered, branch, mod, own)


def solution(mesh):
    return jax.shard_map(
        block,
        mesh=mesh,
        in_specs=(
            P(("sp", "tp"), "dp", None),
            P("sp", "dp", None),
            P("dp", "sp"),
            P("sp"),
            P(),
            P("sp", "tp"),
            P("sp", "tp"),
            P("sp", "tp"),
            P(None, "tp"),
            P(None, "tp"),
            P(None, "tp"),
            P("tp", None),
            P("tp"),
        ),
        out_specs=P(("sp", "tp"), "dp", None),
        check_vma=False,
    )
```

```python
import functools

import jax
import jax.numpy as jnp
import numpy as np
from jax import lax
from jax.experimental import pallas as pl
from jax.experimental.pallas import tpu as pltpu
from jax.sharding import PartitionSpec as P


HEAD_DIM = 128
GRID_W = 64
SEQ = 8192
EPSILON = 1e-06
NEGATIVE = -1e30
LOG2E = 1.4426950408889634

SLOT_REL = (0, 1, 3, 2)
REL_SLOT = (0, 1, 3, 2)

bf16 = jnp.bfloat16
f32 = jnp.float32
VMEM = pltpu.VMEM


def cost(flops, size, exps=0):
    return pl.CostEstimate(flops=int(flops), bytes_accessed=int(size), transcendentals=int(exps))


def in_hbm(array):
    return pltpu.with_memory_space_constraint(array, pltpu.HBM)


def shifted(array, step, axis):
    size = lax.axis_size(axis)
    return lax.ppermute(array, axis, [(i, (i + step) % size) for i in range(size)])


def modulation_kernel(cond_ref, ctx_ref, shift_ref, scale_ref, gate_ref, out_ref, both, rows):
    both[...] = jnp.zeros_like(both)
    both[0:2, :] = cond_ref[...].astype(f32)
    both[2:3, :] = ctx_ref[...].astype(f32)
    raw = both[...]
    act = (raw / (1.0 + jnp.exp(-raw))).astype(bf16)
    rows[0:3, :] = jnp.dot(act, shift_ref[...], preferred_element_type=f32)[0:3]
    rows[3:6, :] = jnp.dot(act, scale_ref[...], preferred_element_type=f32)[0:3]
    rows[6:8, :] = jnp.dot(act, gate_ref[...], preferred_element_type=f32)[0:2]
    for copy in range(out_ref.shape[0]):
        out_ref[copy] = rows[...]


def modulation(copies, condition, ctx_condition, w_shift, w_scale, w_gate):
    depth, width = w_shift.shape
    return pl.pallas_call(
        modulation_kernel,
        out_shape=jax.ShapeDtypeStruct((copies, 8, width), f32),
        scratch_shapes=[VMEM((8, depth), f32), VMEM((8, width), f32)],
        cost_estimate=cost(6e6, 3 * depth * width * 2),
        name="modulation",
        compiler_params=pltpu.CompilerParams(vmem_limit_bytes=4 << 20),
    )(condition, ctx_condition[None], w_shift, w_scale, w_gate)


def modulated_into(h_ref, row, x_ref, where, rows, gain, shift):
    step = 16
    for at in range(0, rows, step):
        x = x_ref[(*where, slice(at, at + step), slice(None))].astype(f32)
        mean = jnp.mean(x * x, axis=-1, keepdims=True)
        h = x * lax.rsqrt(mean + EPSILON) * gain + shift
        h_ref[row + at : row + at + step, :] = h.astype(bf16)


def turned(u, cosine, sine):
    lane = lax.broadcasted_iota(jnp.int32, u.shape, 1)
    swapped = jnp.where(lane % 64 < 32, pltpu.roll(u, 96, 1), pltpu.roll(u, 32, 1))
    return u * cosine + swapped * sine


def project_kernel(*refs):
    own_ref, above_ref, below_ref, across0_ref, across1_ref = refs[:5]
    where_ref, gain_ref, mod_ref, row_cos, row_sin, col_cos, col_sin = refs[5:12]
    wq_ref, wk_ref, wv_ref, q_ref, kv_ref, up_ref, down_ref = refs[12:19]
    x_all, h_ref, w_q, w_kv, q_all, kv_all, sems, out_sems = refs[19:]
    sp, tp = where_ref[0], where_ref[1]
    sources = (
        (own_ref, x_all.at[0]), (above_ref, x_all.at[1]), (below_ref, x_all.at[2]),
        (across0_ref, x_all.at[3, 0]), (across1_ref, x_all.at[3, 1]),
        (wq_ref, w_q), (wk_ref, w_kv.at[:, :HEAD_DIM]), (wv_ref, w_kv.at[:, HEAD_DIM:]),
    )
    copies = [
        pltpu.make_async_copy(source, to, sems.at[i]) for i, (source, to) in enumerate(sources)
    ]
    for copy in copies:
        copy.start()
    gains = [gain_ref[...] * (1.0 + mod_ref[3 + b : 4 + b, :]) for b in range(2)]
    left = lax.broadcasted_iota(jnp.int32, (GRID_W, HEAD_DIM), 1) < HEAD_DIM // 2

    def table(row_ref, col_ref, row):
        parts = [
            jnp.where(left, row_ref[pl.ds(row + i, 1), :], col_ref[...]) for i in range(2)
        ]
        return jnp.concatenate(parts, axis=0)

    chunks = [lax.rem(tp + SLOT_REL[c], 4) for c in range(4)]
    tables = []
    for c in range(4):
        row = sp * 8 + chunks[c] * 2
        tables.append((table(row_cos, col_cos, row), table(row_sin, col_sin, row)))
    for c in range(4):
        for copy in copies[c : c + 1] if c < 3 else copies[3:5]:
            copy.wait()
        for b in range(2):
            shift = mod_ref[b : b + 1, :]
            modulated_into(h_ref.at[c], b * 128, x_all, (c, b), 128, gains[b], shift)
    for copy in copies[5:]:
        copy.wait()
    stores = []
    for n in (2, 0, 1):
        product = jnp.dot(
            h_ref[...].reshape(1024, h_ref.shape[2]),
            w_q[:, n * 256 : n * 256 + 256] if n < 2 else w_kv[...],
            preferred_element_type=f32,
        )
        for c in range(4):
            tok = slice(c * 128, c * 128 + 128)
            for b in range(2):
                rows = slice(c * 256 + b * 128, c * 256 + b * 128 + 128)
                left_part = turned(product[rows, :128], *tables[c]).astype(bf16)
                if n < 2:
                    right_part = turned(product[rows, 128:], *tables[c]).astype(bf16)
                    q_all[2 * n, b, tok, :] = left_part
                    q_all[2 * n + 1, b, tok, :] = right_part
                else:
                    right_part = product[rows, 128:].astype(bf16)
                    kv_all[c, b, 0] = left_part
                    kv_all[c, b, 1] = right_part
        if n < 2:
            stores.append(
                pltpu.make_async_copy(
                    q_all.at[2 * n : 2 * n + 2], q_ref.at[2 * n : 2 * n + 2], out_sems.at[n]
                )
            )
            stores[-1].start()
        else:
            last = (7 - tp) % 4
            first = (4 - tp) % 4
            last = jnp.where(last >= 2, 5 - last, last)
            first = jnp.where(first >= 2, 5 - first, first)
            for i, (source, to) in enumerate(
                ((kv_all.at[last], up_ref), (kv_all.at[first], down_ref), (kv_all, kv_ref))
            ):
                stores.append(pltpu.make_async_copy(source, to, out_sems.at[2 + i]))
                stores[-1].start()
    for store in stores:
        store.wait()


def project(arrays, where, gain, mod, weights):
    width = gain.shape[1]
    whole = pl.BlockSpec(memory_space=VMEM)
    scalars = pl.BlockSpec(memory_space=pltpu.SMEM)
    far = pl.BlockSpec(memory_space=pltpu.HBM)
    shapes = [(4, 2, 512, HEAD_DIM), (4, 2, 2, 128, HEAD_DIM)] + [(2, 2, 128, HEAD_DIM)] * 2
    return pl.pallas_call(
        project_kernel,
        in_specs=[far] * 5 + [scalars] + [whole] * 6 + [far] * 3,
        out_specs=tuple(far for _ in shapes),
        out_shape=tuple(pltpu.HBM(shape, bf16) for shape in shapes),
        scratch_shapes=[
            VMEM((4, 2, 128, width), bf16),
            VMEM((4, 256, width), bf16),
            VMEM((width, 512), bf16),
            VMEM((width, 2 * HEAD_DIM), bf16),
            VMEM(shapes[0], bf16),
            VMEM(shapes[1], bf16),
            pltpu.SemaphoreType.DMA((8,)),
            pltpu.SemaphoreType.DMA((5,)),
        ],
        cost_estimate=cost(2 * 1024 * width * 768, 8e6),
        name="project",
        compiler_params=pltpu.CompilerParams(vmem_limit_bytes=28 << 20),
    )(*map(in_hbm, arrays), where, gain, mod, *rotation_tables(), *map(in_hbm, weights))


def turn_kernel(x_ref, out_ref):
    for b in range(2):
        out_ref[b] = x_ref[:, b, :]


def sample_major(array):
    rows, samples, width = array.shape
    step = rows // 4
    return pl.pallas_call(
        turn_kernel,
        grid=(4,),
        in_specs=[pl.BlockSpec((step, samples, width), lambda i: (i, 0, 0))],
        out_specs=pl.BlockSpec((samples, step, width), lambda i: (0, i, 0)),
        out_shape=pltpu.HBM((samples, rows, width), bf16),
        cost_estimate=cost(0, 4 * array.size),
        name="sample_major",
        compiler_params=pltpu.CompilerParams(vmem_limit_bytes=8 << 20),
    )(in_hbm(array))


def context_kernel(
    x_hbm, where_ref, gain_ref, m0_ref, m1_ref, m2_ref, m3_ref, wk_hbm, wv_hbm,
    out_ref, mod_ref, x_ref, w_kv, h_ref, block, in_sems, sems,
):
    rows = x_ref.shape[1]
    quarter = m0_ref.shape[1]
    loads = [
        pltpu.make_async_copy(source, to, in_sems.at[i])
        for i, (source, to) in enumerate(
            ((x_hbm, x_ref), (wk_hbm, w_kv.at[:, :HEAD_DIM]), (wv_hbm, w_kv.at[:, HEAD_DIM:]))
        )
    ]
    for load in loads:
        load.start()
    for j, m_ref in enumerate((m0_ref, m1_ref, m2_ref, m3_ref)):
        at = pl.multiple_of(lax.rem(where_ref[1] + j, 4) * quarter, quarter)
        mod_ref[:, pl.ds(at, quarter)] = m_ref[...]
    gain = gain_ref[...] * (1.0 + mod_ref[5:6, :])
    shift = mod_ref[2:3, :]
    loads[0].wait()
    for b in range(2):
        modulated_into(h_ref, b * rows, x_ref, (b,), rows, gain, shift)
    for load in loads[1:]:
        load.wait()
    part = jnp.dot(h_ref[...], w_kv[...], preferred_element_type=f32).astype(bf16)
    for b in range(2):
        block[b] = part[b * rows : (b + 1) * rows]
    copies = [
        pltpu.make_async_copy(block, out_ref.at[i], sems.at[i]) for i in range(out_ref.shape[0])
    ]
    for copy in copies:
        copy.start()
    for copy in copies:
        copy.wait()


def project_context(copies, context, where, gain, quarters, w_key, w_value):
    samples, rows, width = context.shape
    whole = pl.BlockSpec(memory_space=VMEM)
    far = pl.BlockSpec(memory_space=pltpu.HBM)
    return pl.pallas_call(
        context_kernel,
        in_specs=[far, pl.BlockSpec(memory_space=pltpu.SMEM)] + [whole] * 5 + [far] * 2,
        out_specs=(far, whole),
        out_shape=(
            pltpu.HBM((copies, samples, rows, 2 * HEAD_DIM), bf16),
            jax.ShapeDtypeStruct((8, width), f32),
        ),
        scratch_shapes=[
            VMEM((samples, rows, width), bf16),
            VMEM((width, 2 * HEAD_DIM), bf16),
            VMEM((samples * rows, width), bf16),
            VMEM((samples, rows, 2 * HEAD_DIM), bf16),
            pltpu.SemaphoreType.DMA((3,)),
            pltpu.SemaphoreType.DMA((copies,)),
        ],
        cost_estimate=cost(2 * 2 * rows * width * 256, 2 * rows * width * 2 + width * 512),
        name="project_context",
        compiler_params=pltpu.CompilerParams(vmem_limit_bytes=10 << 20),
    )(in_hbm(context), where, gain, *quarters, in_hbm(w_key), in_hbm(w_value))


def halves_kernel(below_ref, above_ref, first_ref, second_ref, buffer, sems):
    loads = [
        pltpu.make_async_copy(below_ref.at[0], buffer.at[0], sems.at[0]),
        pltpu.make_async_copy(above_ref.at[1], buffer.at[1], sems.at[1]),
    ]
    stores = [
        pltpu.make_async_copy(buffer.at[0], first_ref, sems.at[2]),
        pltpu.make_async_copy(buffer.at[1], second_ref, sems.at[3]),
    ]
    for load in loads:
        load.start()
    for load, store in zip(loads, stores):
        load.wait()
        store.start()
    for store in stores:
        store.wait()


def halves(below, above):
    far = pl.BlockSpec(memory_space=pltpu.HBM)
    shape = below.shape[1:]
    return pl.pallas_call(
        halves_kernel,
        in_specs=[far] * 2,
        out_specs=(far,) * 2,
        out_shape=(pltpu.HBM(shape, bf16),) * 2,
        scratch_shapes=[VMEM((2, *shape), bf16), pltpu.SemaphoreType.DMA((4,))],
        cost_estimate=cost(0, 4e6),
        name="halves",
        compiler_params=pltpu.CompilerParams(vmem_limit_bytes=4 << 20),
    )(in_hbm(below), in_hbm(above))


def attention_kernel(
    slots, where_ref, sink_ref, q_ref, kv_ref, before_ref, after_ref, ctx_ref, *refs
):
    if slots == (0,):
        w_ref, near, branch_ref, held = refs[0], refs[1:5], refs[5], refs[6:10]
        heads, near_sems = refs[-2:]
        moves = [
            pltpu.make_async_copy(source, to, near_sems.at[i])
            for i, (source, to) in enumerate(zip(near, held))
        ]
        for move in moves:
            move.start()
        outs, refs = (heads,), refs[10:-2]
    else:
        outs, refs = refs[: len(slots)], refs[len(slots) :]
    tile_k, tile_v, keys, values, scores, weights, q_all, kv_all, sems = refs
    copies = [pltpu.make_async_copy(kv_ref, kv_all, sems.at[0])]
    for at, slot in enumerate(slots):
        source = q_ref.at[:, :, slot * 128 : slot * 128 + 128, :]
        copies.append(pltpu.make_async_copy(source, q_all.at[at], sems.at[1 + at]))
    for copy in copies:
        copy.start()
    ctx_len = ctx_ref.shape[0] * ctx_ref.shape[2]
    span = ctx_len + 384
    sp, tp = where_ref[0], where_ref[1]
    ahead = lax.broadcasted_iota(jnp.int32, (128, 128), 1) - lax.broadcasted_iota(
        jnp.int32, (128, 128), 0
    )
    factor = HEAD_DIM ** (-0.5) * LOG2E
    across = (((1,), (1,)), ((), ()))
    values[:, :, HEAD_DIM:] = jnp.ones((2, span, HEAD_DIM), bf16)
    for b in range(2):
        keys[b, :ctx_len, :] = ctx_ref[:, b, :, :HEAD_DIM].reshape(ctx_len, HEAD_DIM)
        values[b, :ctx_len, :HEAD_DIM] = ctx_ref[:, b, :, HEAD_DIM:].reshape(ctx_len, HEAD_DIM)
    for copy in copies:
        copy.wait()
    for b in range(2):
        for tile, which in ((tile_k, 0), (tile_v, 1)):
            for c in range(4):
                tile[b, c * 128 : c * 128 + 128, :] = kv_all[c, b, which]
            tile[b, 512:640, :] = before_ref[b, which]
            tile[b, 640:768, :] = after_ref[b, which]
    units = [(at, slot, b) for at, slot in enumerate(slots) for b in range(2)]
    for at, slot, b in units:
        out_ref = outs[at]
        chunk = lax.rem(tp + SLOT_REL[slot], 4)
        prev = jnp.where(chunk == 0, 4, REL_SLOT[(SLOT_REL[slot] + 3) % 4])
        after = jnp.where(chunk == 3, 5, REL_SLOT[(SLOT_REL[slot] + 1) % 4])
        starts = (pl.multiple_of(prev * 128, 128), slot * 128, pl.multiple_of(after * 128, 128))
        for to, start in enumerate(starts):
            rows = slice(ctx_len + to * 128, ctx_len + to * 128 + 128)
            keys[b, rows, :] = tile_k[b, pl.ds(start, 128), :]
            values[b, rows, :HEAD_DIM] = tile_v[b, pl.ds(start, 128), :]
        q = q_all[at, :, b].reshape(512, HEAD_DIM)
        scores[b] = lax.dot_general(q, keys[b], across, preferred_element_type=f32)
        no_prev = (chunk == 0) & (sp == 0)
        no_after = (chunk == 3) & (sp == SEQ // 512 - 1)
        keep_prev = ahead >= jnp.where(no_prev, 1000, 0)
        keep_after = ahead <= jnp.where(no_after, -1000, 0)
        sinks = []
        for n in range(4):
            rows = slice(n * 128, n * 128 + 128)
            sink = sink_ref[n] * LOG2E

            def part(c):
                tile = scores[b, rows, c * 128 : c * 128 + 128]
                if c == ctx_len // 128:
                    tile = jnp.where(keep_prev, tile, NEGATIVE)
                if c == ctx_len // 128 + 2:
                    tile = jnp.where(keep_after, tile, NEGATIVE)
                return tile

            top = part(0)
            for c in range(1, span // 128):
                top = jnp.maximum(top, part(c))
            top = jnp.maximum(jnp.max(top, axis=-1, keepdims=True) * factor, sink)
            for c in range(span // 128):
                weights[b, rows, c * 128 : c * 128 + 128] = jnp.exp2(
                    part(c) * factor - top
                ).astype(bf16)
            sinks.append(jnp.exp2(sink - top))
        both = jnp.dot(weights[b], values[b], preferred_element_type=f32)
        for n in range(4):
            rows = slice(n * 128, n * 128 + 128)
            total = both[rows, HEAD_DIM:] + sinks[n]
            out_ref[b * 128 : b * 128 + 128, rows] = (
                both[rows, :HEAD_DIM] / total
            ).astype(bf16)
    if slots == (0,):
        part = jnp.dot(heads[...], w_ref[...], preferred_element_type=f32)
        branch_ref[...] = part.astype(bf16)
        for move in moves:
            move.wait()


def attention(slots, where, sink, q, kv, before, after, ctx, w_own=None, near=()):
    parts, _, rows, _ = ctx.shape
    ctx_len = parts * rows
    work = 2 * len(slots) * 4 * 128 * (ctx_len + 384)
    whole = pl.BlockSpec(memory_space=VMEM)
    scalars = pl.BlockSpec(memory_space=pltpu.SMEM)
    operands = [where, sink, in_hbm(q), in_hbm(kv), before, after, ctx]
    in_specs = [scalars] * 2 + [pl.BlockSpec(memory_space=pltpu.HBM)] * 2 + [whole] * 3
    span = ctx_len + 384
    scratch = [
        VMEM((2, 768, HEAD_DIM), bf16),
        VMEM((2, 768, HEAD_DIM), bf16),
        VMEM((2, span, HEAD_DIM), bf16),
        VMEM((2, span, 2 * HEAD_DIM), bf16),
        VMEM((2, 512, span), f32),
        VMEM((2, 512, span), bf16),
        VMEM((len(slots), 4, 2, 128, HEAD_DIM), bf16),
        VMEM(kv.shape, bf16),
        pltpu.SemaphoreType.DMA((1 + len(slots),)),
    ]
    shapes = [(256, 512)] * len(slots)
    if slots == (0,):
        operands += [w_own, *map(in_hbm, near)]
        in_specs += [whole] + [pl.BlockSpec(memory_space=pltpu.HBM)] * len(near)
        shapes = [(256, w_own.shape[1])] + [array.shape for array in near]
        scratch += [VMEM((256, 512), bf16), pltpu.SemaphoreType.DMA((len(near),))]
    return pl.pallas_call(
        functools.partial(attention_kernel, slots),
        in_specs=in_specs,
        out_specs=tuple(whole for _ in shapes),
        out_shape=tuple(jax.ShapeDtypeStruct(shape, bf16) for shape in shapes),
        scratch_shapes=scratch,
        cost_estimate=cost(work * 512, 4e6, work),
        compiler_params=pltpu.CompilerParams(vmem_limit_bytes=24 << 20),
    )(*operands)


def output_kernel(where_ref, *refs):
    a_refs, w_refs = refs[:3], refs[3:11]
    branch_ref, mod_ref, lat_ref, out_ref = refs[11:]
    sp, dp = where_ref[0], where_ref[2]
    odd_x, odd_z = lax.rem(sp, 2), lax.rem(lax.div(sp, 4), 2)
    at_two = []
    for core, odd in ((dp, jnp.where(dp == 0, odd_x, odd_z)), (1 - dp, jnp.where(dp == 0, odd_z, odd_x))):
        at_two += [core * 256 + odd * 128, core * 256 + (1 - odd) * 128]
    groups = (
        (a_refs[0], (2, 6), (dp * 256, 256 - dp * 256)),
        (a_refs[1], (0, 1, 4, 5), at_two),
        (a_refs[2], (3, 7), (dp * 256, 256 - dp * 256)),
    )
    heads = []
    for a_ref, pieces, starts in groups:
        parts = [
            a_ref[:, pl.ds(pl.multiple_of(start, 128), w_refs[i].shape[0])]
            for i, start in zip(pieces, starts)
        ]
        heads.append(jnp.concatenate(parts, axis=1))
    tile = 512
    for n in range(0, out_ref.shape[2], tile):
        cols = slice(n, n + tile)
        total = branch_ref[:, cols].astype(f32)
        for a, (_, pieces, _) in zip(heads, groups):
            w = jnp.concatenate([w_refs[i][:, cols] for i in pieces], axis=0)
            part = jnp.dot(a, w, preferred_element_type=f32)
            total = total + part.astype(bf16).astype(f32)
        for b in range(2):
            gate = mod_ref[6 + b : 7 + b, cols]
            mixed = lat_ref[b, :, cols].astype(f32) + gate * total[b * 128 : b * 128 + 128]
            out_ref[:, b, cols] = mixed.astype(bf16)


def output(where, attn, gathered, branch, mod, latent):
    _, rows, width = latent.shape
    whole = pl.BlockSpec(memory_space=VMEM)
    return pl.pallas_call(
        output_kernel,
        in_specs=[pl.BlockSpec(memory_space=pltpu.SMEM)] + [whole] * (len(attn) + len(gathered) + 3),
        out_specs=whole,
        out_shape=jax.ShapeDtypeStruct((rows, 2, width), bf16),
        cost_estimate=cost(2 * 256 * width * width * 3 // 4, 10e6),
        name="output",
        compiler_params=pltpu.CompilerParams(vmem_limit_bytes=12 << 20),
    )(where, *attn, *gathered, branch, mod, latent)


def rotation_tables():
    quarter = HEAD_DIM // 4
    freqs = np.float32(10000.0) ** (-np.arange(quarter, dtype=np.float32) / np.float32(quarter))
    tables = []
    for count, left in ((SEQ // GRID_W, True), (GRID_W, False)):
        angle = (np.arange(count, dtype=np.float32)[:, None] * freqs).astype(np.float64)
        cosine = np.concatenate([np.cos(angle)] * 2, axis=1)
        sine = np.concatenate([-np.sin(angle), np.sin(angle)], axis=1)
        for values in (cosine, sine):
            pair = [values, np.zeros_like(values)]
            table = np.concatenate(pair if left else pair[::-1], axis=1)
            tables.append(jnp.asarray(table.astype(np.float32)))
    return tables


def block(
    latent, context, condition, ctx_condition, norm_gain, w_shift, w_scale, w_gate,
    w_query, w_key, w_value, w_out, sink,
):
    sp, tp, dp = (lax.axis_index(name) for name in ("sp", "tp", "dp"))
    n_sp = lax.axis_size("sp")
    where = jnp.stack([sp, tp, dp]).astype(jnp.int32)

    own = jnp.moveaxis(latent, 1, 0)
    below = shifted(own, 1, "tp")
    above = shifted(own, -1, "tp")
    first, second = halves(below, above)
    across_0 = shifted(first, 1, "tp")
    across_1 = shifted(second, -1, "tp")

    partial = modulation(n_sp, condition, ctx_condition, w_shift, w_scale, w_gate)
    quarters = lax.all_to_all(partial, "sp", 0, 0, tiled=True)
    quarter = quarters.sum(axis=0)
    around = [quarter]
    for j in (1, 2, 3):
        around.append(shifted(quarter, -j, "tp"))
    gain = norm_gain[None]
    turned_context = sample_major(context)
    ctx, mod = project_context(
        n_sp, turned_context, where, gain, around, w_key, w_value
    )
    ctx = lax.all_to_all(ctx, "sp", 0, 0, tiled=True)

    half = lax.dynamic_slice_in_dim(w_out, dp * 256, 256, axis=0)
    parity = jnp.where(dp == 0, sp % 2, sp // 4 % 2)
    part = lax.dynamic_slice_in_dim(w_out, dp * 256 + parity * 128, 128, axis=0)
    pairs = []
    for s in range(n_sp):
        for d in range(2):
            pairs.append((s * 2 + d, (s ^ (1 if d == 0 else 4)) * 2 + d))
    mine = shifted(part, 2, "tp")
    theirs = lax.ppermute(mine, ("sp", "dp"), pairs)
    w_below = shifted(half, 1, "tp")
    w_above = shifted(half, -1, "tp")
    gathered = [mine, theirs, w_below, w_above]
    for array in tuple(gathered):
        gathered.append(shifted(array, 1, "dp"))

    q, kv, up, down = project(
        (own, above, below, across_0, across_1),
        where, gain, mod, (w_query, w_key, w_value),
    )

    along = [(i, i + 1) for i in range(n_sp - 1)]
    before = lax.ppermute(up, "sp", along)
    after = lax.ppermute(down, "sp", [(j, i) for i, j in along])

    attn = attention((3, 1, 2), where, sink, q, kv, before, after, ctx)
    heads = []
    for j, array in ((1, attn[1]), (2, attn[0]), (3, attn[2])):
        heads.append(shifted(array, j, "tp"))
    branch, *near = attention(
        (0,), where, sink, q, kv, before, after, ctx, w_out, gathered[:4]
    )
    return output(where, heads, near + gathered[4:], branch, mod, own)


def solution(mesh):
    return jax.shard_map(
        block,
        mesh=mesh,
        in_specs=(
            P(("sp", "tp"), "dp", None),
            P("sp", "dp", None),
            P("dp", "sp"),
            P("sp"),
            P(),
            P("sp", "tp"),
            P("sp", "tp"),
            P("sp", "tp"),
            P(None, "tp"),
            P(None, "tp"),
            P(None, "tp"),
            P("tp", None),
            P("tp"),
        ),
        out_specs=P(("sp", "tp"), "dp", None),
        check_vma=False,
    )
```

```python
import functools

import jax
import jax.numpy as jnp
import numpy as np
from jax import lax
from jax.experimental import pallas as pl
from jax.experimental.pallas import tpu as pltpu
from jax.sharding import PartitionSpec as P


HEAD_DIM = 128
GRID_W = 64
SEQ = 8192
EPSILON = 1e-06
NEGATIVE = -1e30
LOG2E = 1.4426950408889634

SLOT_REL = (0, 1, 3, 2)
REL_SLOT = (0, 1, 3, 2)

bf16 = jnp.bfloat16
f32 = jnp.float32
VMEM = pltpu.VMEM


def cost(flops, size, exps=0):
    return pl.CostEstimate(flops=int(flops), bytes_accessed=int(size), transcendentals=int(exps))


def in_hbm(array):
    return pltpu.with_memory_space_constraint(array, pltpu.HBM)


def shifted(array, step, axis):
    size = lax.axis_size(axis)
    return lax.ppermute(array, axis, [(i, (i + step) % size) for i in range(size)])


def modulation_kernel(cond_ref, ctx_ref, shift_ref, scale_ref, gate_ref, out_ref, both, rows):
    both[...] = jnp.zeros_like(both)
    both[0:2, :] = cond_ref[...].astype(f32)
    both[2:3, :] = ctx_ref[...].astype(f32)
    raw = both[...]
    act = (raw / (1.0 + jnp.exp(-raw))).astype(bf16)
    rows[0:3, :] = jnp.dot(act, shift_ref[...], preferred_element_type=f32)[0:3]
    rows[3:6, :] = jnp.dot(act, scale_ref[...], preferred_element_type=f32)[0:3]
    rows[6:8, :] = jnp.dot(act, gate_ref[...], preferred_element_type=f32)[0:2]
    for copy in range(out_ref.shape[0]):
        out_ref[copy] = rows[...]


def modulation(copies, condition, ctx_condition, w_shift, w_scale, w_gate):
    depth, width = w_shift.shape
    return pl.pallas_call(
        modulation_kernel,
        out_shape=jax.ShapeDtypeStruct((copies, 8, width), f32),
        scratch_shapes=[VMEM((8, depth), f32), VMEM((8, width), f32)],
        cost_estimate=cost(6e6, 3 * depth * width * 2),
        name="modulation",
        compiler_params=pltpu.CompilerParams(vmem_limit_bytes=4 << 20),
    )(condition, ctx_condition[None], w_shift, w_scale, w_gate)


def modulated_into(h_ref, row, x_ref, where, rows, gain, shift):
    step = 16
    for at in range(0, rows, step):
        x = x_ref[(*where, slice(at, at + step), slice(None))].astype(f32)
        mean = jnp.mean(x * x, axis=-1, keepdims=True)
        h = x * lax.rsqrt(mean + EPSILON) * gain + shift
        h_ref[row + at : row + at + step, :] = h.astype(bf16)


def turned(u, cosine, sine):
    lane = lax.broadcasted_iota(jnp.int32, u.shape, 1)
    swapped = jnp.where(lane % 64 < 32, pltpu.roll(u, 96, 1), pltpu.roll(u, 32, 1))
    return u * cosine + swapped * sine


def project_kernel(*refs):
    x_refs = refs[:8]
    where_ref, gain_ref, mod_ref, row_cos, row_sin, col_cos, col_sin = refs[8:15]
    wq_ref, wk_ref, wv_ref, q_ref, kv_ref, up_ref, down_ref = refs[15:22]
    x_all, h_ref, w_q, w_kv, q_all, kv_all, sems, out_sems = refs[22:]
    sp, tp = where_ref[0], where_ref[1]
    sources = (
        *((x_ref, x_all.at[i // 2, i % 2]) for i, x_ref in enumerate(x_refs)),
        (wq_ref, w_q), (wk_ref, w_kv.at[:, :HEAD_DIM]), (wv_ref, w_kv.at[:, HEAD_DIM:]),
    )
    copies = [
        pltpu.make_async_copy(source, to, sems.at[i]) for i, (source, to) in enumerate(sources)
    ]
    for copy in copies:
        copy.start()
    gains = [gain_ref[...] * (1.0 + mod_ref[3 + b : 4 + b, :]) for b in range(2)]
    left = lax.broadcasted_iota(jnp.int32, (GRID_W, HEAD_DIM), 1) < HEAD_DIM // 2

    def table(row_ref, col_ref, row):
        parts = [
            jnp.where(left, row_ref[pl.ds(row + i, 1), :], col_ref[...]) for i in range(2)
        ]
        return jnp.concatenate(parts, axis=0)

    chunks = [lax.rem(tp + SLOT_REL[c], 4) for c in range(4)]
    tables = []
    for c in range(4):
        row = sp * 8 + chunks[c] * 2
        tables.append((table(row_cos, col_cos, row), table(row_sin, col_sin, row)))
    for c in range(4):
        for b in range(2):
            copies[2 * c + b].wait()
            shift = mod_ref[b : b + 1, :]
            modulated_into(h_ref.at[c], b * 128, x_all, (c, b), 128, gains[b], shift)
    for copy in copies[8:]:
        copy.wait()
    stores = []
    for n in (2, 0, 1):
        product = jnp.dot(
            h_ref[...].reshape(1024, h_ref.shape[2]),
            w_q[:, n * 256 : n * 256 + 256] if n < 2 else w_kv[...],
            preferred_element_type=f32,
        )
        for c in range(4):
            tok = slice(c * 128, c * 128 + 128)
            for b in range(2):
                rows = slice(c * 256 + b * 128, c * 256 + b * 128 + 128)
                left_part = turned(product[rows, :128], *tables[c]).astype(bf16)
                if n < 2:
                    right_part = turned(product[rows, 128:], *tables[c]).astype(bf16)
                    q_all[2 * n, b, tok, :] = left_part
                    q_all[2 * n + 1, b, tok, :] = right_part
                else:
                    right_part = product[rows, 128:].astype(bf16)
                    kv_all[c, b, 0] = left_part
                    kv_all[c, b, 1] = right_part
        if n < 2:
            stores.append(
                pltpu.make_async_copy(
                    q_all.at[2 * n : 2 * n + 2], q_ref.at[2 * n : 2 * n + 2], out_sems.at[n]
                )
            )
            stores[-1].start()
        else:
            last = (7 - tp) % 4
            first = (4 - tp) % 4
            last = jnp.where(last >= 2, 5 - last, last)
            first = jnp.where(first >= 2, 5 - first, first)
            for i, (source, to) in enumerate(
                ((kv_all.at[last], up_ref), (kv_all.at[first], down_ref), (kv_all, kv_ref))
            ):
                stores.append(pltpu.make_async_copy(source, to, out_sems.at[2 + i]))
                stores[-1].start()
    for store in stores:
        store.wait()


def project(arrays, where, gain, mod, weights):
    width = gain.shape[1]
    whole = pl.BlockSpec(memory_space=VMEM)
    scalars = pl.BlockSpec(memory_space=pltpu.SMEM)
    far = pl.BlockSpec(memory_space=pltpu.HBM)
    shapes = [(4, 2, 512, HEAD_DIM), (4, 2, 2, 128, HEAD_DIM)] + [(2, 2, 128, HEAD_DIM)] * 2
    return pl.pallas_call(
        project_kernel,
        in_specs=[far] * 8 + [scalars] + [whole] * 6 + [far] * 3,
        out_specs=tuple(far for _ in shapes),
        out_shape=tuple(pltpu.HBM(shape, bf16) for shape in shapes),
        scratch_shapes=[
            VMEM((4, 2, 128, width), bf16),
            VMEM((4, 256, width), bf16),
            VMEM((width, 512), bf16),
            VMEM((width, 2 * HEAD_DIM), bf16),
            VMEM(shapes[0], bf16),
            VMEM(shapes[1], bf16),
            pltpu.SemaphoreType.DMA((11,)),
            pltpu.SemaphoreType.DMA((5,)),
        ],
        cost_estimate=cost(2 * 1024 * width * 768, 8e6),
        name="project",
        compiler_params=pltpu.CompilerParams(vmem_limit_bytes=28 << 20),
    )(*map(in_hbm, arrays), where, gain, mod, *rotation_tables(), *map(in_hbm, weights))


def context_kernel(
    x_hbm, where_ref, gain_ref, m0_ref, m1_ref, m2_ref, m3_ref, wk_hbm, wv_hbm,
    out_ref, mod_ref, x_ref, w_kv, h_ref, block, in_sems, sems,
):
    rows = x_ref.shape[1]
    quarter = m0_ref.shape[1]
    loads = [
        pltpu.make_async_copy(source, to, in_sems.at[i])
        for i, (source, to) in enumerate(
            ((x_hbm, x_ref), (wk_hbm, w_kv.at[:, :HEAD_DIM]), (wv_hbm, w_kv.at[:, HEAD_DIM:]))
        )
    ]
    for load in loads:
        load.start()
    for j, m_ref in enumerate((m0_ref, m1_ref, m2_ref, m3_ref)):
        at = pl.multiple_of(lax.rem(where_ref[1] + j, 4) * quarter, quarter)
        mod_ref[:, pl.ds(at, quarter)] = m_ref[...]
    gain = gain_ref[...] * (1.0 + mod_ref[5:6, :])
    shift = mod_ref[2:3, :]
    loads[0].wait()
    for b in range(2):
        modulated_into(h_ref, b * rows, x_ref, (b,), rows, gain, shift)
    for load in loads[1:]:
        load.wait()
    part = jnp.dot(h_ref[...], w_kv[...], preferred_element_type=f32).astype(bf16)
    for b in range(2):
        block[b] = part[b * rows : (b + 1) * rows]
    copies = [
        pltpu.make_async_copy(block, out_ref.at[i], sems.at[i]) for i in range(out_ref.shape[0])
    ]
    for copy in copies:
        copy.start()
    for copy in copies:
        copy.wait()


def project_context(copies, context, where, gain, quarters, w_key, w_value):
    samples, rows, width = context.shape
    whole = pl.BlockSpec(memory_space=VMEM)
    far = pl.BlockSpec(memory_space=pltpu.HBM)
    return pl.pallas_call(
        context_kernel,
        in_specs=[far, pl.BlockSpec(memory_space=pltpu.SMEM)] + [whole] * 5 + [far] * 2,
        out_specs=(far, whole),
        out_shape=(
            pltpu.HBM((copies, samples, rows, 2 * HEAD_DIM), bf16),
            jax.ShapeDtypeStruct((8, width), f32),
        ),
        scratch_shapes=[
            VMEM((samples, rows, width), bf16),
            VMEM((width, 2 * HEAD_DIM), bf16),
            VMEM((samples * rows, width), bf16),
            VMEM((samples, rows, 2 * HEAD_DIM), bf16),
            pltpu.SemaphoreType.DMA((3,)),
            pltpu.SemaphoreType.DMA((copies,)),
        ],
        cost_estimate=cost(2 * 2 * rows * width * 256, 2 * rows * width * 2 + width * 512),
        name="project_context",
        compiler_params=pltpu.CompilerParams(vmem_limit_bytes=10 << 20),
    )(in_hbm(context), where, gain, *quarters, in_hbm(w_key), in_hbm(w_value))


def halves_kernel(own_ref, first_ref, second_ref, buffer, sems):
    loads = [
        pltpu.make_async_copy(own_ref.at[b], buffer.at[b], sems.at[b]) for b in range(2)
    ]
    stores = [
        pltpu.make_async_copy(buffer.at[0], first_ref, sems.at[2]),
        pltpu.make_async_copy(buffer.at[1], second_ref, sems.at[3]),
    ]
    for load in loads:
        load.start()
    for load, store in zip(loads, stores):
        load.wait()
        store.start()
    for store in stores:
        store.wait()


def halves(own):
    far = pl.BlockSpec(memory_space=pltpu.HBM)
    shape = own.shape[1:]
    return pl.pallas_call(
        halves_kernel,
        in_specs=[far],
        out_specs=(far,) * 2,
        out_shape=(pltpu.HBM(shape, bf16),) * 2,
        scratch_shapes=[VMEM((2, *shape), bf16), pltpu.SemaphoreType.DMA((4,))],
        cost_estimate=cost(0, 4e6),
        name="halves",
        compiler_params=pltpu.CompilerParams(vmem_limit_bytes=4 << 20),
    )(in_hbm(own))


def attention_kernel(
    slots, where_ref, sink_ref, q_ref, kv_ref, before_ref, after_ref, ctx_ref, *refs
):
    if slots == (0,):
        w_ref, near, branch_ref, held = refs[0], refs[1:5], refs[5], refs[6:10]
        heads, near_sems = refs[-2:]
        moves = [
            pltpu.make_async_copy(source, to, near_sems.at[i])
            for i, (source, to) in enumerate(zip(near, held))
        ]
        for move in moves:
            move.start()
        outs, refs = (heads,), refs[10:-2]
    else:
        outs, refs = refs[: len(slots)], refs[len(slots) :]
    tile_k, tile_v, keys, values, scores, weights, q_all, kv_all, sems = refs
    copies = [pltpu.make_async_copy(kv_ref, kv_all, sems.at[0])]
    for at, slot in enumerate(slots):
        source = q_ref.at[:, :, slot * 128 : slot * 128 + 128, :]
        copies.append(pltpu.make_async_copy(source, q_all.at[at], sems.at[1 + at]))
    for copy in copies:
        copy.start()
    ctx_len = ctx_ref.shape[0] * ctx_ref.shape[2]
    span = ctx_len + 384
    sp, tp = where_ref[0], where_ref[1]
    ahead = lax.broadcasted_iota(jnp.int32, (128, 128), 1) - lax.broadcasted_iota(
        jnp.int32, (128, 128), 0
    )
    factor = HEAD_DIM ** (-0.5) * LOG2E
    across = (((1,), (1,)), ((), ()))
    values[:, :, HEAD_DIM:] = jnp.ones((2, span, HEAD_DIM), bf16)
    for b in range(2):
        keys[b, :ctx_len, :] = ctx_ref[:, b, :, :HEAD_DIM].reshape(ctx_len, HEAD_DIM)
        values[b, :ctx_len, :HEAD_DIM] = ctx_ref[:, b, :, HEAD_DIM:].reshape(ctx_len, HEAD_DIM)
    for copy in copies:
        copy.wait()
    for b in range(2):
        for tile, which in ((tile_k, 0), (tile_v, 1)):
            for c in range(4):
                tile[b, c * 128 : c * 128 + 128, :] = kv_all[c, b, which]
            tile[b, 512:640, :] = before_ref[b, which]
            tile[b, 640:768, :] = after_ref[b, which]
    units = [(at, slot, b) for at, slot in enumerate(slots) for b in range(2)]
    for at, slot, b in units:
        out_ref = outs[at]
        chunk = lax.rem(tp + SLOT_REL[slot], 4)
        prev = jnp.where(chunk == 0, 4, REL_SLOT[(SLOT_REL[slot] + 3) % 4])
        after = jnp.where(chunk == 3, 5, REL_SLOT[(SLOT_REL[slot] + 1) % 4])
        starts = (pl.multiple_of(prev * 128, 128), slot * 128, pl.multiple_of(after * 128, 128))
        for to, start in enumerate(starts):
            rows = slice(ctx_len + to * 128, ctx_len + to * 128 + 128)
            keys[b, rows, :] = tile_k[b, pl.ds(start, 128), :]
            values[b, rows, :HEAD_DIM] = tile_v[b, pl.ds(start, 128), :]
        q = q_all[at, :, b].reshape(512, HEAD_DIM)
        scores[b] = lax.dot_general(q, keys[b], across, preferred_element_type=f32)
        no_prev = (chunk == 0) & (sp == 0)
        no_after = (chunk == 3) & (sp == SEQ // 512 - 1)
        keep_prev = ahead >= jnp.where(no_prev, 1000, 0)
        keep_after = ahead <= jnp.where(no_after, -1000, 0)
        sinks = []
        for n in range(4):
            rows = slice(n * 128, n * 128 + 128)
            sink = sink_ref[n] * LOG2E

            def part(c):
                tile = scores[b, rows, c * 128 : c * 128 + 128]
                if c == ctx_len // 128:
                    tile = jnp.where(keep_prev, tile, NEGATIVE)
                if c == ctx_len // 128 + 2:
                    tile = jnp.where(keep_after, tile, NEGATIVE)
                return tile

            top = part(0)
            for c in range(1, span // 128):
                top = jnp.maximum(top, part(c))
            top = jnp.maximum(jnp.max(top, axis=-1, keepdims=True) * factor, sink)
            for c in range(span // 128):
                weights[b, rows, c * 128 : c * 128 + 128] = jnp.exp2(
                    part(c) * factor - top
                ).astype(bf16)
            sinks.append(jnp.exp2(sink - top))
        both = jnp.dot(weights[b], values[b], preferred_element_type=f32)
        for n in range(4):
            rows = slice(n * 128, n * 128 + 128)
            total = both[rows, HEAD_DIM:] + sinks[n]
            out_ref[b * 128 : b * 128 + 128, rows] = (
                both[rows, :HEAD_DIM] / total
            ).astype(bf16)
    if slots == (0,):
        part = jnp.dot(heads[...], w_ref[...], preferred_element_type=f32)
        branch_ref[...] = part.astype(bf16)
        for move in moves:
            move.wait()


def attention(slots, where, sink, q, kv, before, after, ctx, w_own=None, near=()):
    parts, _, rows, _ = ctx.shape
    ctx_len = parts * rows
    work = 2 * len(slots) * 4 * 128 * (ctx_len + 384)
    whole = pl.BlockSpec(memory_space=VMEM)
    scalars = pl.BlockSpec(memory_space=pltpu.SMEM)
    operands = [where, sink, in_hbm(q), in_hbm(kv), before, after, ctx]
    in_specs = [scalars] * 2 + [pl.BlockSpec(memory_space=pltpu.HBM)] * 2 + [whole] * 3
    span = ctx_len + 384
    scratch = [
        VMEM((2, 768, HEAD_DIM), bf16),
        VMEM((2, 768, HEAD_DIM), bf16),
        VMEM((2, span, HEAD_DIM), bf16),
        VMEM((2, span, 2 * HEAD_DIM), bf16),
        VMEM((2, 512, span), f32),
        VMEM((2, 512, span), bf16),
        VMEM((len(slots), 4, 2, 128, HEAD_DIM), bf16),
        VMEM(kv.shape, bf16),
        pltpu.SemaphoreType.DMA((1 + len(slots),)),
    ]
    shapes = [(256, 512)] * len(slots)
    if slots == (0,):
        operands += [w_own, *map(in_hbm, near)]
        in_specs += [whole] + [pl.BlockSpec(memory_space=pltpu.HBM)] * len(near)
        shapes = [(256, w_own.shape[1])] + [array.shape for array in near]
        scratch += [VMEM((256, 512), bf16), pltpu.SemaphoreType.DMA((len(near),))]
    return pl.pallas_call(
        functools.partial(attention_kernel, slots),
        in_specs=in_specs,
        out_specs=tuple(whole for _ in shapes),
        out_shape=tuple(jax.ShapeDtypeStruct(shape, bf16) for shape in shapes),
        scratch_shapes=scratch,
        cost_estimate=cost(work * 512, 4e6, work),
        compiler_params=pltpu.CompilerParams(vmem_limit_bytes=24 << 20),
    )(*operands)


def output_kernel(where_ref, *refs):
    a_refs, w_refs = refs[:3], refs[3:11]
    branch_ref, mod_ref, lat_ref, out_ref = refs[11:]
    sp, dp = where_ref[0], where_ref[2]
    odd_x, odd_z = lax.rem(sp, 2), lax.rem(lax.div(sp, 4), 2)
    at_two = []
    for core, odd in ((dp, jnp.where(dp == 0, odd_x, odd_z)), (1 - dp, jnp.where(dp == 0, odd_z, odd_x))):
        at_two += [core * 256 + odd * 128, core * 256 + (1 - odd) * 128]
    groups = (
        (a_refs[0], (2, 6), (dp * 256, 256 - dp * 256)),
        (a_refs[1], (0, 1, 4, 5), at_two),
        (a_refs[2], (3, 7), (dp * 256, 256 - dp * 256)),
    )
    heads = []
    for a_ref, pieces, starts in groups:
        parts = [
            a_ref[:, pl.ds(pl.multiple_of(start, 128), w_refs[i].shape[0])]
            for i, start in zip(pieces, starts)
        ]
        heads.append(jnp.concatenate(parts, axis=1))
    tile = 512
    for n in range(0, out_ref.shape[2], tile):
        cols = slice(n, n + tile)
        total = branch_ref[:, cols].astype(f32)
        for a, (_, pieces, _) in zip(heads, groups):
            w = jnp.concatenate([w_refs[i][:, cols] for i in pieces], axis=0)
            part = jnp.dot(a, w, preferred_element_type=f32)
            total = total + part.astype(bf16).astype(f32)
        for b in range(2):
            gate = mod_ref[6 + b : 7 + b, cols]
            mixed = lat_ref[b, :, cols].astype(f32) + gate * total[b * 128 : b * 128 + 128]
            out_ref[:, b, cols] = mixed.astype(bf16)


def output(where, attn, gathered, branch, mod, latent):
    _, rows, width = latent.shape
    whole = pl.BlockSpec(memory_space=VMEM)
    return pl.pallas_call(
        output_kernel,
        in_specs=[pl.BlockSpec(memory_space=pltpu.SMEM)] + [whole] * (len(attn) + len(gathered) + 3),
        out_specs=whole,
        out_shape=jax.ShapeDtypeStruct((rows, 2, width), bf16),
        cost_estimate=cost(2 * 256 * width * width * 3 // 4, 10e6),
        name="output",
        compiler_params=pltpu.CompilerParams(vmem_limit_bytes=12 << 20),
    )(where, *attn, *gathered, branch, mod, latent)


def rotation_tables():
    quarter = HEAD_DIM // 4
    freqs = np.float32(10000.0) ** (-np.arange(quarter, dtype=np.float32) / np.float32(quarter))
    tables = []
    for count, left in ((SEQ // GRID_W, True), (GRID_W, False)):
        angle = (np.arange(count, dtype=np.float32)[:, None] * freqs).astype(np.float64)
        cosine = np.concatenate([np.cos(angle)] * 2, axis=1)
        sine = np.concatenate([-np.sin(angle), np.sin(angle)], axis=1)
        for values in (cosine, sine):
            pair = [values, np.zeros_like(values)]
            table = np.concatenate(pair if left else pair[::-1], axis=1)
            tables.append(jnp.asarray(table.astype(np.float32)))
    return tables


def block(
    latent, context, condition, ctx_condition, norm_gain, w_shift, w_scale, w_gate,
    w_query, w_key, w_value, w_out, sink,
):
    sp, tp, dp = (lax.axis_index(name) for name in ("sp", "tp", "dp"))
    n_sp = lax.axis_size("sp")
    where = jnp.stack([sp, tp, dp]).astype(jnp.int32)

    own = jnp.moveaxis(latent, 1, 0)
    own_0, own_1 = halves(own)
    below_0 = shifted(own_0, 1, "tp")
    above_1 = shifted(own_1, -1, "tp")
    below_1 = shifted(own_1, 1, "tp")
    above_0 = shifted(own_0, -1, "tp")
    across_0 = shifted(below_0, 1, "tp")
    across_1 = shifted(above_1, -1, "tp")

    partial = modulation(n_sp, condition, ctx_condition, w_shift, w_scale, w_gate)
    quarters = lax.all_to_all(partial, "sp", 0, 0, tiled=True)
    quarter = quarters.sum(axis=0)
    around = [quarter]
    for j in (1, 2, 3):
        around.append(shifted(quarter, -j, "tp"))
    gain = norm_gain[None]
    turned_context = jnp.moveaxis(context, 1, 0)
    ctx, mod = project_context(
        n_sp, turned_context, where, gain, around, w_key, w_value
    )
    ctx = lax.all_to_all(ctx, "sp", 0, 0, tiled=True)

    half = lax.dynamic_slice_in_dim(w_out, dp * 256, 256, axis=0)
    parity = jnp.where(dp == 0, sp % 2, sp // 4 % 2)
    part = lax.dynamic_slice_in_dim(w_out, dp * 256 + parity * 128, 128, axis=0)
    pairs = []
    for s in range(n_sp):
        for d in range(2):
            pairs.append((s * 2 + d, (s ^ (1 if d == 0 else 4)) * 2 + d))
    mine = shifted(part, 2, "tp")
    theirs = lax.ppermute(mine, ("sp", "dp"), pairs)
    w_below = shifted(half, 1, "tp")
    w_above = shifted(half, -1, "tp")
    gathered = [mine, theirs, w_below, w_above]
    for array in tuple(gathered):
        gathered.append(shifted(array, 1, "dp"))

    q, kv, up, down = project(
        (own_0, own_1, above_0, above_1, below_0, below_1, across_0, across_1),
        where, gain, mod, (w_query, w_key, w_value),
    )

    along = [(i, i + 1) for i in range(n_sp - 1)]
    before = lax.ppermute(up, "sp", along)
    after = lax.ppermute(down, "sp", [(j, i) for i, j in along])

    attn = attention((3, 1, 2), where, sink, q, kv, before, after, ctx)
    heads = []
    for j, array in ((1, attn[1]), (2, attn[0]), (3, attn[2])):
        heads.append(shifted(array, j, "tp"))
    branch, *near = attention(
        (0,), where, sink, q, kv, before, after, ctx, w_out, gathered[:4]
    )
    return output(where, heads, near + gathered[4:], branch, mod, own)


def solution(mesh):
    return jax.shard_map(
        block,
        mesh=mesh,
        in_specs=(
            P(("sp", "tp"), "dp", None),
            P("sp", "dp", None),
            P("dp", "sp"),
            P("sp"),
            P(),
            P("sp", "tp"),
            P("sp", "tp"),
            P("sp", "tp"),
            P(None, "tp"),
            P(None, "tp"),
            P(None, "tp"),
            P("tp", None),
            P("tp"),
        ),
        out_specs=P(("sp", "tp"), "dp", None),
        check_vma=False,
    )
```
